768 devices in a mesh: fs: 24 (over z, core), tp: 32 (over y, x).
Axes of the slice: x: 4, y: 8, z: 12, core: 2. Of those that a mesh axis runs over, the one named last changes fastest.
Arguments:
- trained_gate: float32 [32, 504, 2048], P(None, 'fs', 'tp'), may hold values from -0.125 to 0.125
- trained_up: float32 [32, 504, 2048], P(None, 'fs', 'tp'), may hold values from -0.125 to 0.125
- trained_down: float32 [32, 504, 2048], P(None, 'fs', 'tp'), may hold values from -0.25 to 0.25
- trained_shared_gate: float32 [504, 2048], P('fs', 'tp'), may hold values from -0.125 to 0.125
- trained_shared_up: float32 [504, 2048], P('fs', 'tp'), may hold values from -0.125 to 0.125
- trained_shared_down: float32 [504, 2048], P('fs', 'tp'), may hold values from -0.25 to 0.25
- ffn_gain: float32 [2048], P('tp'), may hold values from 0.1 to 1.9
- prompt_tokens: bfloat16 [6144, 2048], P('fs'), may hold values from -6 to 6
- expert_ids: int32 [6144, 8], P('fs'), may hold values from 0 to 31, all different within a row; in each aligned block of 256 rows (0 to 255, 256 to 511, ...) at most 160 rows name the same one
- route_scores: float32 [6144, 8], P('fs'), may hold values from 0.05 to 1
Outputs:
- served_gate: bfloat16 [32, 504, 2048], P('tp')
- served_up: bfloat16 [32, 504, 2048], P('tp')
- served_down: bfloat16 [32, 504, 2048], P('tp')
- served_shared_gate: bfloat16 [504, 2048], P(None, 'tp')
- served_shared_up: bfloat16 [504, 2048], P(None, 'tp')
- served_shared_down: bfloat16 [504, 2048], P(None, 'tp')
- mixture_out: bfloat16 [6144, 2048], P('fs', 'tp')
The draws below stay inside these ranges and needn't reach their ends.
Inputs may be any that keep to these rules, and one draw needn't show every extreme that they name: `expert_ids`: each row names 8 different experts, and every expert is named by some row. Within the 256 rows of one index of fs no expert is named by more than 160 rows, and in every draw some expert is named by exactly 160 rows of some index of fs.
All inputs are finite; a program needn't handle non-finite values.
Results may differ from the reference program's by a relative error of at most 0.0082.
Values may be sent and summed in bfloat16 or wider, within the bound.
A program may use at most 64 MiB of HBM per device.

```python
import math
import jax
import jax.numpy as jnp
import numpy as np
from jax import lax

D = 2048
FF = 504
TOP_K = 8
TOK = 256
EXPERTS = 32
CAP = 160
TOKENS = 6144
N_FS = 24


def level_of(key, shape, split, low, largest):
    gain = 1.0
    for axis_at, parts in split:
        heights = jax.random.uniform(jax.random.fold_in(jax.random.fold_in(key, 6), axis_at), (parts,), jnp.float32, low / len(split), largest / len(split))
        gain = gain * jnp.repeat(jnp.exp(heights), shape[axis_at] // parts).reshape((-1,) + (1,) * (len(shape) - 1 - axis_at))
    return gain


def assign_block(key, own, number, rows, count, top, reach, lean):
    order = jax.random.permutation(key, count)
    crowded, common = shares(count, rows * top, reach, lean, True), shares(count, rows * top, reach, lean, False)
    places = jnp.arange(count)

    def named(lengths, rotation):
        used = int((lengths > 0).sum())
        fixed = max(1, used // 4)
        moved = fixed + (places - fixed + rotation * (used - fixed)) % max(1, count - fixed)
        return jnp.zeros((count,), jnp.int32).at[order[jnp.where(places < fixed, places, moved)]].set(jnp.asarray(lengths, jnp.int32))

    lengths = jnp.where(number % 4 == 0, named(crowded, number // 4), named(common, number - number // 4 - 1))
    mixed = jax.random.permutation(jax.random.fold_in(own, 3), count)
    donor, sink = mixed[0:count // 2 * 2:2], mixed[1:count // 2 * 2:2]
    slack = jnp.minimum(lengths[donor] - 1, reach - lengths[sink]) // 2
    slack = jnp.where((donor == order[0]) | (sink == order[0]) | (lengths[sink] == 0), 0, jnp.maximum(slack, 0))
    moved = jax.random.randint(jax.random.fold_in(own, 4), (count // 2,), 0, 1 << 20) % (slack + 1)
    lengths = lengths.at[donor].add(-moved).at[sink].add(moved)
    labels = jnp.searchsorted(jnp.cumsum(lengths), jnp.arange(rows * top), side="right").astype(jnp.int32)
    table = labels.reshape(top, rows).T
    table = table[jax.random.permutation(jax.random.fold_in(own, 1), rows)]
    rotation = jax.random.randint(jax.random.fold_in(own, 2), (rows, 1), 0, top)
    return jnp.take_along_axis(table, (jnp.arange(top)[None, :] + rotation) % top, axis=1)


def shares(count, total, most, lean, full):
    portions = [(1 << 20) // math.isqrt(rank ** lean) + 1 for rank in range(1, count + 1)]
    largest = most if full else min(most, max(-(-total // count), total * portions[0] // sum(portions)))
    least = 1 if total - largest >= count - 1 else 0
    counts, rest = [largest] + [least] * (count - 1), total - largest - least * (count - 1)
    while rest > 0:
        movable = [i for i in range(1, count) if counts[i] < largest] or [i for i in range(1, count) if counts[i] < most]
        mass, budget = sum([portions[i] for i in movable]), rest
        for i in movable:
            addition = min(most - counts[i], max(1, budget * portions[i] // mass), rest)
            counts[i] = counts[i] + addition
            rest = rest - addition
    return np.array(counts)


def scatter_about(key, shape, width, most, cuts=(), held_as=jnp.bfloat16):
    entries = width * jax.random.normal(key, shape, jnp.float32)
    if cuts:
        entries = entries * level_of(key, shape, cuts, -0.22, 0.18)
    return jnp.clip(entries, -most, most).astype(held_as)


def setup_inputs(seed: int = 0) -> dict:
    seeds = jax.random.split(jax.random.key(seed), 11)
    trained_gate = scatter_about(seeds[0], (EXPERTS, FF, D), D ** -0.5, 0.125, ((1, 24), (2, 32)), jnp.float32)
    trained_up = scatter_about(seeds[1], (EXPERTS, FF, D), D ** -0.5, 0.125, ((1, 24), (2, 32)), jnp.float32)
    trained_down = scatter_about(seeds[2], (EXPERTS, FF, D), FF ** -0.5, 0.25, ((1, 24), (2, 32)), jnp.float32)
    trained_shared_gate = scatter_about(seeds[3], (FF, D), D ** -0.5, 0.125, ((0, 24), (1, 32)), jnp.float32)
    trained_shared_up = scatter_about(seeds[4], (FF, D), D ** -0.5, 0.125, ((0, 24), (1, 32)), jnp.float32)
    trained_shared_down = scatter_about(seeds[5], (FF, D), FF ** -0.5, 0.25, ((0, 24), (1, 32)), jnp.float32)
    ffn_gain = jnp.clip(1.0 + 0.18 * jax.random.normal(seeds[6], (D,), jnp.float32), 0.1, 1.9)
    prompt_tokens = scatter_about(seeds[7], (TOKENS, D), 1.0, 6.0, ((0, 24),))
    expert_ids_keys = jax.random.split(jax.random.fold_in(seeds[8], 1), TOKENS // TOK)
    expert_ids_turns = jax.random.permutation(jax.random.fold_in(seeds[8], 3), TOKENS // TOK)
    expert_ids = jax.vmap(lambda own, number: assign_block(jax.random.fold_in(seeds[8], 2), own, number, TOK, EXPERTS, TOP_K, CAP, 1))(expert_ids_keys, expert_ids_turns).reshape((TOKENS, TOP_K))
    route_scores = jnp.clip(jnp.exp(math.log(1.0) - 2.9957323 * jax.random.uniform(seeds[9], (TOKENS, TOP_K), jnp.float32) ** level_of(seeds[9], (TOKENS, TOP_K), ((0, 24),), -0.2, 0.2)), 0.05, 1.0)
    return {"trained_gate": trained_gate, "trained_up": trained_up, "trained_down": trained_down, "trained_shared_gate": trained_shared_gate, "trained_shared_up": trained_shared_up, "trained_shared_down": trained_shared_down, "ffn_gain": ffn_gain, "prompt_tokens": prompt_tokens, "expert_ids": expert_ids, "route_scores": route_scores}


EPSILON = 1e-06
ROUTED_SCALE = 2.5

def contract(left, right):
    return lax.dot_general(left, right, (((1,), (1,)), ((), ())), preferred_element_type=jnp.float32)

def reference(trained_gate, trained_up, trained_down, trained_shared_gate, trained_shared_up, trained_shared_down, ffn_gain, prompt_tokens, expert_ids, route_scores):
    served_gate = (trained_gate * ffn_gain[None, None, :]).astype(jnp.bfloat16)
    served_up = (trained_up * ffn_gain[None, None, :]).astype(jnp.bfloat16)
    served_down = trained_down.astype(jnp.bfloat16)
    served_shared_gate = (trained_shared_gate * ffn_gain[None, :]).astype(jnp.bfloat16)
    served_shared_up = (trained_shared_up * ffn_gain[None, :]).astype(jnp.bfloat16)
    served_shared_down = trained_shared_down.astype(jnp.bfloat16)
    tokens_float = prompt_tokens.astype(jnp.float32)
    normed = (tokens_float * lax.rsqrt(lax.optimization_barrier(jnp.mean(tokens_float * tokens_float, axis=1, keepdims=True)) + EPSILON)).astype(jnp.bfloat16)
    route_weight = ROUTED_SCALE * route_scores / lax.optimization_barrier(jnp.sum(route_scores, axis=1, keepdims=True))
    token_total = prompt_tokens.shape[0]
    slot_total = N_FS * CAP
    token_range = jnp.arange(token_total, dtype=jnp.int32)

    def one_expert(routed, inputs):
        expert_index, gate_weight, up_weight, down_weight = inputs
        chosen = expert_ids == expert_index
        token_weight = lax.optimization_barrier(jnp.sum(jnp.where(chosen, route_weight, 0.0), axis=1))
        present = jnp.any(chosen, axis=1)
        position = (jnp.cumsum(present.astype(jnp.int32)) - 1).astype(jnp.int32)
        target = jnp.where(present, position, slot_total).astype(jnp.int32)
        slot_token = jnp.zeros((slot_total + 1,), jnp.int32).at[target].set(token_range)[:slot_total]
        slot_rows = jnp.take(normed, slot_token, axis=0)
        gate_pre = contract(slot_rows, gate_weight)
        up_pre = contract(slot_rows, up_weight)
        expert_act = (jax.nn.silu(gate_pre) * up_pre).astype(jnp.bfloat16)
        expert_out = jnp.dot(expert_act, down_weight, preferred_element_type=jnp.float32)
        picked = jnp.take(expert_out, jnp.maximum(position, 0), axis=0)
        return (routed + jnp.where(present[:, None], picked * token_weight[:, None], 0.0), None)
    expert_range = jnp.arange(EXPERTS, dtype=jnp.int32)
    routed, _ = lax.scan(one_expert, jnp.zeros((token_total, D), jnp.float32), (expert_range, served_gate, served_up, served_down))
    shared_gate_pre = contract(normed, served_shared_gate)
    shared_up_pre = contract(normed, served_shared_up)
    shared_act = (jax.nn.silu(shared_gate_pre) * shared_up_pre).astype(jnp.bfloat16)
    shared_out = jnp.dot(shared_act, served_shared_down, preferred_element_type=jnp.float32)
    mixture_out = (routed + shared_out).astype(jnp.bfloat16)
    return (served_gate, served_up, served_down, served_shared_gate, served_shared_up, served_shared_down, mixture_out)
```

```python
import functools

import jax
import jax.numpy as jnp
from jax import lax
from jax.experimental import pallas as pl
from jax.experimental.pallas import tpu as pltpu
from jax.sharding import PartitionSpec as P

EPSILON = 1e-06
ROUTED_SCALE = 2.5
MESH = pl.DeviceIdType.MESH
NX = 4
CHUNKS = 4
ROW = 64
F32, BF16 = jnp.float32, jnp.bfloat16


def nt(a, b):
    return lax.dot_general(a, b, (((1,), (1,)), ((), ())), preferred_element_type=F32)


def tn(a, b):
    return lax.dot_general(a, b, (((0,), (0,)), ((), ())), preferred_element_type=F32)


def nn(a, b):
    return jnp.dot(a, b, preferred_element_type=F32)


def iota(shape, dim):
    return lax.broadcasted_iota(jnp.int32, shape, dim)


def silu(v):
    return v / (1.0 + jnp.exp(-v))


def halves(a, b):
    low = iota(a.shape, len(a.shape) - 1) < 64
    ax = len(a.shape) - 1
    return (
        jnp.where(low, a, pltpu.roll(b, 64, ax)),
        jnp.where(low, pltpu.roll(a, 64, ax), b),
    )


def kernel(
    n_tp, nz, units, cap,
    tg, tu, td, sg, su, sd, gain, tok, ids, scores,
    o_gate, o_up, o_down, o_sgate, o_sup, o_sdown, o_mix,
    send_a, recv_a, blocks, small, normed, rows, total, spread, slot_weight,
    pre_send, pre_recv, acts, sdown, send_x, recv_x, send_y, recv_y, staged,
    sem_a, sem_ring_s, sem_ring_r, sem_pair_s, sem_pair_r,
    sem_small_s, sem_small_r, sem_spair, sem_j, sem_act, sem_x_s, sem_x_r, sem_y_s, sem_y_r,
    sem_out,
):
    n_y = n_tp // NX
    far = nz // 2
    groups = nz // 4
    group_rows = 8 * units
    hidden = nz * 2 * units
    per_j = pre_send.shape[1]
    width = total.shape[1]
    tokens = tok.shape[0]
    me = lax.axis_index("tp")
    fs = lax.axis_index("fs")
    z, core = fs // 2, lax.rem(fs, 2)
    y, x = me // NX, lax.rem(me, NX)
    ahead = lax.rem(z + 1, nz) * 2 + core
    behind = lax.rem(z + nz - 1, nz) * 2 + core
    twin = z * 2 + 1 - core

    barrier = pltpu.get_barrier_semaphore()

    def greet(i, _):
        peer = lax.rem(me + i, n_tp)
        pl.semaphore_signal(barrier, inc=1, device_id={"tp": peer}, device_id_type=MESH)
        return 0

    for other in (ahead, behind, twin):
        pl.semaphore_signal(barrier, inc=1, device_id={"fs": other}, device_id_type=MESH)
    lax.fori_loop(1, n_tp, greet, 0)

    def pack(g, u, d):
        stack = jnp.concatenate([g, u, d, jnp.zeros((ROW - 3 * units, 64), F32)], axis=0)
        return jnp.concatenate([stack[: ROW // 2], stack[ROW // 2 :]], axis=1).astype(BF16)

    scale = gain[...]

    def prepare(e, _):
        send_a[e] = pack(tg[e] * scale, tu[e] * scale, td[e])
        return 0

    small[z, core] = pack(sg[...] * scale, su[...] * scale, sd[...])
    lax.fori_loop(0, n_tp, prepare, 0)
    recv_a[me] = send_a[me]
    pl.semaphore_wait(barrier, n_tp + 2)

    def plane(src, dst, sems, peer):
        return pltpu.make_async_remote_copy(
            src_ref=src, dst_ref=dst, send_sem=sems.at[0], recv_sem=sems.at[1],
            device_id={"tp": peer}, device_id_type=MESH,
        )

    def plane_done(ref, sems):
        piece = ref.at[pl.ds(0, n_tp - 1)]
        done = plane(piece, piece, sems, lax.rem(me + 1, n_tp))
        done.wait_send()
        done.wait_recv()

    def small_hop(d, s, at):
        return pltpu.make_async_remote_copy(
            src_ref=small.at[at, core], dst_ref=small.at[at, core],
            send_sem=sem_small_s.at[d, s], recv_sem=sem_small_r.at[d, s],
            device_id={"fs": ahead if d == 0 else behind}, device_id_type=MESH,
        )

    def small_pair(at):
        return pltpu.make_async_remote_copy(
            src_ref=small.at[at, core], dst_ref=small.at[at, core],
            send_sem=sem_spair.at[0], recv_sem=sem_spair.at[1],
            device_id={"fs": twin}, device_id_type=MESH,
        )

    def origin(d, s):
        return lax.rem(z + nz - s, nz) if d == 0 else lax.rem(z + s, nz)

    small_hop(0, 1, z).start()
    small_hop(1, 1, z).start()
    small_pair(z).start()

    def send_weights(i, _):
        peer = lax.rem(me + i, n_tp)
        plane(send_a.at[peer], recv_a.at[me], sem_a, peer).start()
        return 0

    lax.fori_loop(1, n_tp, send_weights, 0)

    def small_step(s):
        for d in (0, 1):

            def arrived(d=d):
                at = origin(d, s)
                small_hop(d, s, at).wait_recv()
                small_pair(at).start()

                @pl.when((s + 1 < far) | ((s + 1 == far) & (d == 0)))
                def _():
                    small_hop(d, s + 1, at).start()

            if d == 0:
                arrived()
            else:
                pl.when(s < far)(arrived)

    tf = tok[...].astype(F32)
    normed[...] = (
        tf * lax.rsqrt(jnp.mean(tf * tf, axis=1, keepdims=True) + EPSILON)
    ).astype(BF16)
    ids_v, sc = ids[...], scores[...]
    ratio = ROUTED_SCALE * sc / jnp.sum(sc, axis=1, keepdims=True)
    lane = iota((tokens, 128), 1)
    present = jnp.zeros((tokens, 128), F32)
    weight = jnp.zeros((tokens, 128), F32)
    for k in range(ids.shape[1]):
        hit = ids_v[:, k : k + 1] == lane
        present = jnp.where(hit, 1.0, present)
        weight = jnp.where(hit, weight + ratio[:, k : k + 1], weight)
    before = jnp.where(iota((tokens, tokens), 1) < iota((tokens, tokens), 0), 1.0, 0.0)
    position = nn(before.astype(BF16), present.astype(BF16))
    slot = jnp.where(present > 0.0, position, -1.0)
    mine = iota((128, tokens), 0) == me
    slot_row = jnp.sum(jnp.where(mine, slot.T, 0.0), axis=0, keepdims=True)
    weight_row = jnp.sum(jnp.where(mine, weight.T, 0.0), axis=0, keepdims=True)
    taken = slot_row == iota((cap, tokens), 0).astype(F32)
    slot_weight[...] = jnp.broadcast_to(
        jnp.sum(jnp.where(taken, weight_row, 0.0), axis=1, keepdims=True), slot_weight.shape
    )
    rows[...] = nn(jnp.where(taken, 1.0, 0.0).astype(BF16), normed[...]).astype(BF16)
    for i in range(NX):
        col = jnp.sum(jnp.where(lane == y * NX + i, slot, 0.0), axis=1, keepdims=True)
        spread[i] = jnp.where(col == iota((tokens, cap), 1).astype(F32), 1.0, 0.0).astype(BF16)
    total[...] = jnp.zeros_like(total)

    small_step(1)
    plane_done(recv_a, sem_a)

    for m in range(n_tp // 2):
        top, low = halves(recv_a[2 * m].astype(F32), recv_a[2 * m + 1].astype(F32))
        whole = jnp.concatenate([top, low], axis=0)
        blocks[z, core, :, pl.ds(128 * m, 128)] = whole.astype(BF16)

    size = ROW // CHUNKS

    def hop(d, s, q, at):
        piece = blocks.at[at, core, pl.ds(q * size, size)]
        return pltpu.make_async_remote_copy(
            src_ref=piece, dst_ref=piece,
            send_sem=sem_ring_s.at[d, s, q], recv_sem=sem_ring_r.at[d, s, q],
            device_id={"fs": ahead if d == 0 else behind}, device_id_type=MESH,
        )

    def pair(at):
        rel = lax.rem(at + nz - z, nz)
        return pltpu.make_async_remote_copy(
            src_ref=blocks.at[at, core], dst_ref=blocks.at[at, core],
            send_sem=sem_pair_s.at[rel], recv_sem=sem_pair_r.at[rel],
            device_id={"fs": twin}, device_id_type=MESH,
        )

    for q in range(CHUNKS):
        for d in (0, 1):
            hop(d, 1, q, z).start()
    pair(z).start()

    def last_leg(d, q):
        return (q < CHUNKS // 2) == (d == 0)

    def expert(at):
        pair(at).wait_recv()
        w = blocks[at].reshape(2 * ROW, width)
        pre = nt(rows[...], w)
        act = silu(pltpu.roll(pre, 2 * units, 1)) * pltpu.roll(pre, units, 1)
        unit = iota(act.shape, 1) & (ROW - 1)
        act = jnp.where((unit >= 2 * units) & (unit < 3 * units), act, 0.0).astype(BF16)
        total[...] += nn(act, w)

    def picks():
        shape = (group_rows, 8 * ROW)
        i, c = iota(shape, 0), iota(shape, 1)
        f, r = c // ROW, c & (ROW - 1)
        return [
            jnp.where((r >= units * m) & (r < units * (m + 1)) & (i == units * f + r - units * m), 1.0, 0.0).astype(BF16)
            for m in range(3)
        ]

    def shared_rows():
        def spent(i, _):
            small_pair(z).wait_recv()
            return 0

        got = [[], [], []]
        for g in range(groups):
            v = small[pl.ds(4 * g, 4)].reshape(8, ROW // 2, 128).astype(F32)
            v = jnp.concatenate([v, pltpu.roll(v, 64, 2)], axis=1).reshape(8 * ROW, 128)
            v = v.astype(BF16)
            for m, p in enumerate(picks()):
                got[m].append(nn(p, v))
        gate, up, down = [jnp.concatenate(one, axis=0) for one in got]
        for o, v in ((o_sgate, gate), (o_sup, up), (o_sdown, down)):
            o[...] = v[:, :64].astype(BF16)
        pad = jnp.zeros((n_tp * per_j - hidden, 128), F32)
        both = jnp.concatenate([halves(gate, up)[0], pad], axis=0)
        pre_send[...] = both.astype(BF16).reshape(n_tp, per_j, 128)
        low = iota(down.shape, 1) < 64
        down = jnp.concatenate([jnp.where(low, down, 0.0), pad], axis=0)
        sdown[...] = down.astype(BF16)
        pre_recv[me] = pre_send[me]

        def send(i, _):
            peer = lax.rem(me + i, n_tp)
            plane(pre_send.at[peer], pre_recv.at[me], sem_j, peer).start()
            return 0

        lax.fori_loop(1, n_tp, send, 0)

    def ring_step(s, _):
        for q in range(CHUNKS):
            for d in (0, 1):

                def arrived(d=d, q=q):
                    at = origin(d, s)
                    hop(d, s, q, at).wait_recv()
                    go = s + 1 <= far if last_leg(d, q) else s + 1 < far

                    @pl.when(go)
                    def _():
                        hop(d, s + 1, q, at).start()

                if last_leg(d, q):
                    arrived()
                else:
                    pl.when(s < far)(arrived)
        pair(origin(0, s)).start()

        @pl.when(s < far)
        def _():
            pair(origin(1, s)).start()

        @pl.when(s < far)
        def _():
            small_step(s + 1)

        def one(i, _):
            expert(lax.rem(z + nz + (s - 1) * (1 - 2 * i), nz))
            return 0

        lax.fori_loop(0, jnp.where(s == 1, 1, 2), one, 0)

        @pl.when(s == far)
        def _():
            everything = small.at[:, 0]
            done = pltpu.make_async_remote_copy(
                src_ref=everything, dst_ref=everything,
                send_sem=sem_spair.at[0], recv_sem=sem_spair.at[1],
                device_id={"fs": twin}, device_id_type=MESH,
            )
            done.wait_send()
            done.wait_recv()
            shared_rows()

        return 0

    lax.fori_loop(1, far + 1, ring_step, 0)
    expert(lax.rem(z + far, nz))

    w = slot_weight[...]
    for p in range(n_y // 2):
        for h in range(NX // 2):
            a = total[:, pl.ds(128 * (2 * p * (NX // 2) + h), 128)] * w
            b = total[:, pl.ds(128 * ((2 * p + 1) * (NX // 2) + h), 128)] * w
            left, right = halves(a, b)
            send_x[2 * h, :, pl.ds(128 * p, 128)] = left.astype(BF16)
            send_x[2 * h + 1, :, pl.ds(128 * p, 128)] = right.astype(BF16)

    def row_copy(i):
        to = lax.rem(x + i, NX)
        return pltpu.make_async_remote_copy(
            src_ref=send_x.at[to], dst_ref=recv_x.at[x],
            send_sem=sem_x_s.at[i], recv_sem=sem_x_r.at[i],
            device_id={"tp": y * NX + to}, device_id_type=MESH,
        )

    for i in range(1, NX):
        row_copy(i).start()
    recv_x[x] = send_x[x]

    plane_done(pre_recv, sem_j)
    gates, ups = [], []
    for m in range(n_tp // 2):
        g, u = halves(pre_recv[2 * m].astype(F32), pre_recv[2 * m + 1].astype(F32))
        gates.append(g.astype(BF16))
        ups.append(u.astype(BF16))
    gate = nt(jnp.concatenate(gates, axis=1), normed[...])
    up = nt(jnp.concatenate(ups, axis=1), normed[...])
    acts[me] = (silu(gate) * up).astype(BF16)

    def send_act(i, _):
        peer = lax.rem(me + i, n_tp)
        plane(acts.at[me], acts.at[me], sem_act, peer).start()
        return 0

    lax.fori_loop(1, n_tp, send_act, 0)

    part = min(512, width)
    steps = width // part
    outs = (o_gate, o_up, o_down)

    def leave(m, g):
        return pltpu.make_async_copy(staged.at[m, g], outs[m].at[g], sem_out.at[m, g])

    for g in range(groups):
        for m, p in enumerate(picks()):

            def served(n, _, m=m, g=g, p=p):
                cols = pl.ds(pl.multiple_of(n * part, part), part)
                v = blocks[pl.ds(4 * g, 4), :, :, cols].reshape(8 * ROW, part)
                staged[m, g, :, cols] = nn(p, v).astype(BF16)
                return 0

            lax.fori_loop(0, steps, served, 0)
            leave(m, g).start()

    for i in range(1, NX):
        row_copy(i).wait_send()
        row_copy(i).wait_recv()

    half = tokens // 2
    for p in range(n_y // 2):
        acc = jnp.zeros((tokens, 128), F32)
        for i in range(NX):
            acc += nn(spread[i], recv_x[i, :, pl.ds(128 * p, 128)])
        left, right = halves(acc[:half], acc[half:])
        send_y[2 * p] = left.astype(BF16)
        send_y[2 * p + 1] = right.astype(BF16)

    def col_copy(i):
        to = lax.rem(y + i, n_y)
        return pltpu.make_async_remote_copy(
            src_ref=send_y.at[to], dst_ref=recv_y.at[y],
            send_sem=sem_y_s.at[i], recv_sem=sem_y_r.at[i],
            device_id={"tp": to * NX + x}, device_id_type=MESH,
        )

    for i in range(1, n_y):
        col_copy(i).start()
    recv_y[y] = send_y[y]

    def act_done():
        piece = acts.at[pl.ds(0, n_tp - 1)]
        done = plane(piece, piece, sem_act, lax.rem(me + 1, n_tp))
        done.wait_send()
        done.wait_recv()

    act_done()
    shared = tn(acts[...].reshape(n_tp * per_j, tokens), sdown[...])
    mixed = halves(shared[:half], shared[half:])[0]
    for i in range(1, n_y):
        col_copy(i).wait_send()
        col_copy(i).wait_recv()
    for i in range(n_y):
        mixed += recv_y[i].astype(F32)
    upper = pltpu.roll(mixed, 64, 1)
    o_mix[...] = jnp.concatenate([mixed[:, :64], upper[:, :64]], axis=0).astype(BF16)

    for d in (0, 1):
        for q in range(CHUNKS):

            def sent(s, _, d=d, q=q):
                hop(d, s, q, z).wait_send()
                return 0

            lax.fori_loop(1, far + (1 if last_leg(d, q) else 0), sent, 0)

        def small_sent(s, _, d=d):
            small_hop(d, s, z).wait_send()
            return 0

        lax.fori_loop(1, far + (1 if d == 0 else 0), small_sent, 0)

    def pair_sent(i, _):
        pair(i).wait_send()
        return 0

    lax.fori_loop(0, nz, pair_sent, 0)
    for g in range(groups):
        for m in range(3):
            leave(m, g).wait()


def on_device(*args):
    tg, ids = args[0], args[8]
    n_tp, units = tg.shape[0], tg.shape[1]
    nz = lax.axis_size("fs") // 2
    tokens, width = args[7].shape
    top = ids.shape[1]
    cap = min(tokens, 5 * tokens * top // (2 * n_tp))
    hidden = nz * 2 * units
    per_j = -(-hidden // (16 * n_tp)) * 16
    n_y = n_tp // NX
    far = nz // 2
    groups = nz // 4
    args = list(args)
    args[6] = args[6].reshape(1, -1)
    vm = pl.BlockSpec(memory_space=pltpu.VMEM)
    hbm = pl.BlockSpec(memory_space=pl.ANY)
    dma = pltpu.SemaphoreType.DMA
    big = jax.ShapeDtypeStruct((groups, 8 * units, width), BF16)
    thin = jax.ShapeDtypeStruct((hidden, 64), BF16)
    outs = pl.pallas_call(
        functools.partial(kernel, n_tp, nz, units, cap),
        name="hand_over",
        out_shape=[big, big, big, thin, thin, thin, jax.ShapeDtypeStruct((tokens, 64), BF16)],
        in_specs=[vm] * 10,
        out_specs=[hbm] * 3 + [vm] * 4,
        scratch_shapes=[
            pltpu.VMEM((n_tp, ROW // 2, 128), BF16),
            pltpu.VMEM((n_tp, ROW // 2, 128), BF16),
            pltpu.VMEM((nz, 2, ROW, width), BF16),
            pltpu.VMEM((nz, 2, ROW // 2, 128), BF16),
            pltpu.VMEM((tokens, width), BF16),
            pltpu.VMEM((cap, width), BF16),
            pltpu.VMEM((cap, width), F32),
            pltpu.VMEM((NX, tokens, cap), BF16),
            pltpu.VMEM((cap, 128), F32),
            pltpu.VMEM((n_tp, per_j, 128), BF16),
            pltpu.VMEM((n_tp, per_j, 128), BF16),
            pltpu.VMEM((n_tp, per_j, tokens), BF16),
            pltpu.VMEM((n_tp * per_j, 128), BF16),
            pltpu.VMEM((NX, cap, 64 * n_y), BF16),
            pltpu.VMEM((NX, cap, 64 * n_y), BF16),
            pltpu.VMEM((n_y, tokens // 2, 128), BF16),
            pltpu.VMEM((n_y, tokens // 2, 128), BF16),
            pltpu.VMEM((3, groups, 8 * units, width), BF16),
            dma((2,)),
            dma((2, far + 1, CHUNKS)),
            dma((2, far + 1, CHUNKS)),
            dma((nz,)),
            dma((nz,)),
            dma((2, far + 1)),
            dma((2, far + 1)),
            dma((2,)),
            dma((2,)),
            dma((2,)),
            dma((NX,)),
            dma((NX,)),
            dma((n_y,)),
            dma((n_y,)),
            dma((3, groups)),
        ],
        compiler_params=pltpu.CompilerParams(
            collective_id=0, has_side_effects=True, vmem_limit_bytes=56 * 1024 * 1024
        ),
    )(*args)
    gate, up, down, sgate, sup, sdown, mixture = outs
    full = [v.reshape(1, hidden, width) for v in (gate, up, down)]
    return (*full, sgate, sup, sdown, mixture)


def solution(mesh):
    placed = (
        P(None, "fs", "tp"),
        P(None, "fs", "tp"),
        P(None, "fs", "tp"),
        P("fs", "tp"),
        P("fs", "tp"),
        P("fs", "tp"),
        P("tp"),
        P("fs", None),
        P("fs", None),
        P("fs", None),
    )
    return jax.shard_map(
        on_device,
        mesh=mesh,
        in_specs=placed,
        out_specs=(
            P("tp", None, None),
            P("tp", None, None),
            P("tp", None, None),
            P(None, "tp"),
            P(None, "tp"),
            P(None, "tp"),
            P("fs", "tp"),
        ),
        check_vma=False,
    )
```

```python
import functools

import jax
import jax.numpy as jnp
from jax import lax
from jax.experimental import pallas as pl
from jax.experimental.pallas import tpu as pltpu
from jax.sharding import PartitionSpec as P

EPSILON = 1e-06
ROUTED_SCALE = 2.5
MESH = pl.DeviceIdType.MESH
NX = 4
CHUNKS = 4
ROW = 64
F32, BF16 = jnp.float32, jnp.bfloat16


def nt(a, b):
    return lax.dot_general(a, b, (((1,), (1,)), ((), ())), preferred_element_type=F32)


def tn(a, b):
    return lax.dot_general(a, b, (((0,), (0,)), ((), ())), preferred_element_type=F32)


def nn(a, b):
    return jnp.dot(a, b, preferred_element_type=F32)


def iota(shape, dim):
    return lax.broadcasted_iota(jnp.int32, shape, dim)


def silu(v):
    return v / (1.0 + jnp.exp(-v))


def halves(a, b):
    low = iota(a.shape, len(a.shape) - 1) < 64
    ax = len(a.shape) - 1
    return (
        jnp.where(low, a, pltpu.roll(b, 64, ax)),
        jnp.where(low, pltpu.roll(a, 64, ax), b),
    )


def kernel(
    n_tp, nz, units, cap,
    tg, tu, td, sg, su, sd, gain, tok, ids, scores,
    o_gate, o_up, o_down, o_sgate, o_sup, o_sdown, o_mix,
    packed, send_a, recv_a, blocks, small, normed, rows, total, spread, slot_weight,
    pre_send, pre_recv, acts, sdown, send_x, recv_x, send_y, recv_y,
    sem_a, sem_ring_s, sem_ring_r, sem_pair_s, sem_pair_r,
    sem_small_s, sem_small_r, sem_spair, sem_j, sem_act, sem_x_s, sem_x_r, sem_y_s, sem_y_r,
):
    n_y = n_tp // NX
    far = nz // 2
    groups = nz // 4
    group_rows = 8 * units
    hidden = nz * 2 * units
    per_j = pre_send.shape[1]
    width = total.shape[1]
    tokens = tok.shape[0]
    me = lax.axis_index("tp")
    fs = lax.axis_index("fs")
    z, core = fs // 2, lax.rem(fs, 2)
    y, x = me // NX, lax.rem(me, NX)
    ahead = lax.rem(z + 1, nz) * 2 + core
    behind = lax.rem(z + nz - 1, nz) * 2 + core
    twin = z * 2 + 1 - core

    barrier = pltpu.get_barrier_semaphore()

    def greet(i, _):
        peer = lax.rem(me + i, n_tp)
        pl.semaphore_signal(barrier, inc=1, device_id={"tp": peer}, device_id_type=MESH)
        return 0

    for other in (ahead, behind, twin):
        pl.semaphore_signal(barrier, inc=1, device_id={"fs": other}, device_id_type=MESH)
    lax.fori_loop(1, n_tp, greet, 0)

    scale = gain[...]

    with jax.named_scope("pack"):

        def unit(r):
            if r < units:
                return tg[r] * scale
            if r < 2 * units:
                return tu[r - units] * scale
            return td[r - 2 * units] if r < 3 * units else jnp.zeros((n_tp, 64), F32)

        parts = [sg[...] * scale, su[...] * scale, sd[...]]
        stack = jnp.concatenate([*parts, jnp.zeros((ROW - 3 * units, 64), F32)], axis=0)
        stack = jnp.concatenate([stack[: ROW // 2], stack[ROW // 2 :]], axis=1)
        small[z, core] = stack.astype(BF16)
        for r in range(0, ROW // 2, 8):
            several = [
                jnp.concatenate([unit(i), unit(i + ROW // 2)], axis=1) for i in range(r, r + 8)
            ]
            packed[:, pl.ds(r, 8), :] = jnp.swapaxes(jnp.stack(several, axis=0), 0, 1)
        send_a[...] = packed[...].astype(BF16)
        recv_a[me] = send_a[me]
    with jax.named_scope("entry"):
        pl.semaphore_wait(barrier, n_tp + 2)

    def plane(src, dst, sems, peer):
        return pltpu.make_async_remote_copy(
            src_ref=src, dst_ref=dst, send_sem=sems.at[0], recv_sem=sems.at[1],
            device_id={"tp": peer}, device_id_type=MESH,
        )

    def plane_done(ref, sems):
        piece = ref.at[pl.ds(0, n_tp - 1)]
        done = plane(piece, piece, sems, lax.rem(me + 1, n_tp))
        done.wait_send()
        done.wait_recv()

    def small_hop(d, s, at):
        return pltpu.make_async_remote_copy(
            src_ref=small.at[at, core], dst_ref=small.at[at, core],
            send_sem=sem_small_s.at[d, s], recv_sem=sem_small_r.at[d, s],
            device_id={"fs": ahead if d == 0 else behind}, device_id_type=MESH,
        )

    def small_pair(at):
        return pltpu.make_async_remote_copy(
            src_ref=small.at[at, core], dst_ref=small.at[at, core],
            send_sem=sem_spair.at[0], recv_sem=sem_spair.at[1],
            device_id={"fs": twin}, device_id_type=MESH,
        )

    def origin(d, s):
        return lax.rem(z + nz - s, nz) if d == 0 else lax.rem(z + s, nz)

    small_hop(0, 1, z).start()
    small_hop(1, 1, z).start()
    small_pair(z).start()

    def send_weights(i, _):
        peer = lax.rem(me + i, n_tp)
        plane(send_a.at[peer], recv_a.at[me], sem_a, peer).start()
        return 0

    lax.fori_loop(1, n_tp, send_weights, 0)

    def small_step(s):
        for d in (0, 1):

            def arrived(d=d):
                at = origin(d, s)
                small_hop(d, s, at).wait_recv()
                small_pair(at).start()

                @pl.when((s + 1 < far) | ((s + 1 == far) & (d == 0)))
                def _():
                    small_hop(d, s + 1, at).start()

            if d == 0:
                arrived()
            else:
                pl.when(s < far)(arrived)

    tf = tok[...].astype(F32)
    normed[...] = (
        tf * lax.rsqrt(jnp.mean(tf * tf, axis=1, keepdims=True) + EPSILON)
    ).astype(BF16)
    ids_v, sc = ids[...], scores[...]
    ratio = ROUTED_SCALE * sc / jnp.sum(sc, axis=0, keepdims=True)
    expert_row = iota((128, tokens), 0)
    present = jnp.zeros((128, tokens), F32)
    weight_row = jnp.zeros((1, tokens), F32)
    for k in range(ids.shape[0]):
        present = jnp.where(ids_v[k : k + 1] == expert_row, 1.0, present)
        weight_row += jnp.where(ids_v[k : k + 1] == me, ratio[k : k + 1], 0.0)
    before = jnp.where(iota((tokens, tokens), 0) < iota((tokens, tokens), 1), 1.0, 0.0)
    position = nn(present.astype(BF16), before.astype(BF16))
    slots = jnp.where(present > 0.0, position, -1.0)
    slot_row = jnp.sum(jnp.where(expert_row == me, slots, 0.0), axis=0, keepdims=True)
    slot = slots.T
    lane = iota((tokens, 128), 1)
    taken = slot_row == iota((cap, tokens), 0).astype(F32)
    slot_weight[...] = jnp.broadcast_to(
        jnp.sum(jnp.where(taken, weight_row, 0.0), axis=1, keepdims=True), slot_weight.shape
    )
    rows[...] = nn(jnp.where(taken, 1.0, 0.0).astype(BF16), normed[...]).astype(BF16)
    for i in range(NX):
        col = jnp.sum(jnp.where(lane == y * NX + i, slot, 0.0), axis=1, keepdims=True)
        spread[i] = jnp.where(col == iota((tokens, cap), 1).astype(F32), 1.0, 0.0).astype(BF16)
    total[...] = jnp.zeros_like(total)

    small_step(1)
    plane_done(recv_a, sem_a)

    for m in range(n_tp // 2):
        top, low = halves(recv_a[2 * m].astype(F32), recv_a[2 * m + 1].astype(F32))
        whole = jnp.concatenate([top, low], axis=0)
        blocks[z, core, :, pl.ds(128 * m, 128)] = whole.astype(BF16)

    size = ROW // CHUNKS

    def hop(d, s, q, at):
        piece = blocks.at[at, core, pl.ds(q * size, size)]
        return pltpu.make_async_remote_copy(
            src_ref=piece, dst_ref=piece,
            send_sem=sem_ring_s.at[d, s, q], recv_sem=sem_ring_r.at[d, s, q],
            device_id={"fs": ahead if d == 0 else behind}, device_id_type=MESH,
        )

    def pair(at):
        rel = lax.rem(at + nz - z, nz)
        return pltpu.make_async_remote_copy(
            src_ref=blocks.at[at, core], dst_ref=blocks.at[at, core],
            send_sem=sem_pair_s.at[rel], recv_sem=sem_pair_r.at[rel],
            device_id={"fs": twin}, device_id_type=MESH,
        )

    for q in range(CHUNKS):
        for d in (0, 1):
            hop(d, 1, q, z).start()
    pair(z).start()

    def last_leg(d, q):
        return (q < CHUNKS // 2) == (d == 0)

    def expert(at):
        pair(at).wait_recv()
        w = blocks[at].reshape(2 * ROW, width)
        pre = nt(rows[...], w)
        act = silu(pltpu.roll(pre, 2 * units, 1)) * pltpu.roll(pre, units, 1)
        unit = iota(act.shape, 1) & (ROW - 1)
        act = jnp.where((unit >= 2 * units) & (unit < 3 * units), act, 0.0).astype(BF16)
        total[...] += nn(act, w)

    def picks():
        shape = (group_rows, 8 * ROW)
        i, c = iota(shape, 0), iota(shape, 1)
        f, r = c // ROW, c & (ROW - 1)
        return [
            jnp.where((r >= units * m) & (r < units * (m + 1)) & (i == units * f + r - units * m), 1.0, 0.0).astype(BF16)
            for m in range(3)
        ]

    def padded(v):
        spare = jnp.zeros((-hidden % 128, 128), F32)
        return jnp.concatenate([v, spare], axis=0)

    def shared_rows():
        got = [[], [], []]
        for g in range(groups):
            v = small[pl.ds(4 * g, 4)].reshape(8, ROW // 2, 128).astype(F32)
            v = jnp.concatenate([v, pltpu.roll(v, 64, 2)], axis=1).reshape(8 * ROW, 128)
            v = v.astype(BF16)
            for m, p in enumerate(picks()):
                got[m].append(nn(p, v))
        gate, up, down = [jnp.concatenate(one, axis=0) for one in got]
        for o, v in ((o_sgate, gate), (o_sup, up), (o_sdown, down)):
            o[...] = padded(v).T[:64, :hidden].astype(BF16)
        pad = jnp.zeros((n_tp * per_j - hidden, 128), F32)
        both = jnp.concatenate([halves(gate, up)[0], pad], axis=0)
        pre_send[...] = both.astype(BF16).reshape(n_tp, per_j, 128)
        low = iota(down.shape, 1) < 64
        down = jnp.concatenate([jnp.where(low, down, 0.0), pad], axis=0)
        sdown[...] = down.astype(BF16)
        pre_recv[me] = pre_send[me]

        def send(i, _):
            peer = lax.rem(me + i, n_tp)
            plane(pre_send.at[peer], pre_recv.at[me], sem_j, peer).start()
            return 0

        lax.fori_loop(1, n_tp, send, 0)

    def ring_step(s, _):
        for q in range(CHUNKS):
            for d in (0, 1):

                def arrived(d=d, q=q):
                    at = origin(d, s)
                    hop(d, s, q, at).wait_recv()
                    go = s + 1 <= far if last_leg(d, q) else s + 1 < far

                    @pl.when(go)
                    def _():
                        hop(d, s + 1, q, at).start()

                if last_leg(d, q):
                    arrived()
                else:
                    pl.when(s < far)(arrived)
        pair(origin(0, s)).start()

        @pl.when(s < far)
        def _():
            pair(origin(1, s)).start()

        @pl.when(s < far)
        def _():
            small_step(s + 1)

        def one(i, _):
            expert(lax.rem(z + nz + (s - 1) * (1 - 2 * i), nz))
            return 0

        lax.fori_loop(0, jnp.where(s == 1, 1, 2), one, 0)

        @pl.when(s == far)
        def _():
            everything = small.at[:, 0]
            done = pltpu.make_async_remote_copy(
                src_ref=everything, dst_ref=everything,
                send_sem=sem_spair.at[0], recv_sem=sem_spair.at[1],
                device_id={"fs": twin}, device_id_type=MESH,
            )
            done.wait_send()
            done.wait_recv()
            shared_rows()

        return 0

    lax.fori_loop(1, far + 1, ring_step, 0)
    expert(lax.rem(z + far, nz))

    w = slot_weight[...]
    for p in range(n_y // 2):
        for h in range(NX // 2):
            a = total[:, pl.ds(128 * (2 * p * (NX // 2) + h), 128)] * w
            b = total[:, pl.ds(128 * ((2 * p + 1) * (NX // 2) + h), 128)] * w
            left, right = halves(a, b)
            send_x[2 * h, :, pl.ds(128 * p, 128)] = left.astype(BF16)
            send_x[2 * h + 1, :, pl.ds(128 * p, 128)] = right.astype(BF16)

    def row_copy(i):
        to = lax.rem(x + i, NX)
        return pltpu.make_async_remote_copy(
            src_ref=send_x.at[to], dst_ref=recv_x.at[x],
            send_sem=sem_x_s.at[i], recv_sem=sem_x_r.at[i],
            device_id={"tp": y * NX + to}, device_id_type=MESH,
        )

    for i in range(1, NX):
        row_copy(i).start()
    recv_x[x] = send_x[x]

    plane_done(pre_recv, sem_j)
    gates, ups = [], []
    for m in range(n_tp // 2):
        g, u = halves(pre_recv[2 * m].astype(F32), pre_recv[2 * m + 1].astype(F32))
        gates.append(g.astype(BF16))
        ups.append(u.astype(BF16))
    gate = nt(jnp.concatenate(gates, axis=1), normed[...])
    up = nt(jnp.concatenate(ups, axis=1), normed[...])
    acts[me] = (silu(gate) * up).astype(BF16)

    def send_act(i, _):
        peer = lax.rem(me + i, n_tp)
        plane(acts.at[me], acts.at[me], sem_act, peer).start()
        return 0

    lax.fori_loop(1, n_tp, send_act, 0)

    part = min(512, width)
    steps = width // part
    outs = (o_gate, o_up, o_down)

    for g in range(groups):
        for m, p in enumerate(picks()):

            def served(n, _, m=m, g=g, p=p):
                cols = pl.ds(pl.multiple_of(n * part, part), part)
                v = blocks[pl.ds(4 * g, 4), :, :, cols].reshape(8 * ROW, part)
                outs[m][g, :, cols] = nn(p, v).astype(BF16)
                return 0

            lax.fori_loop(0, steps, served, 0)

    for i in range(1, NX):
        row_copy(i).wait_send()
        row_copy(i).wait_recv()

    half = tokens // 2
    for p in range(n_y // 2):
        acc = jnp.zeros((tokens, 128), F32)
        for i in range(NX):
            acc += nn(spread[i], recv_x[i, :, pl.ds(128 * p, 128)])
        left, right = halves(acc[:half], acc[half:])
        send_y[2 * p] = left.astype(BF16)
        send_y[2 * p + 1] = right.astype(BF16)

    def col_copy(i):
        to = lax.rem(y + i, n_y)
        return pltpu.make_async_remote_copy(
            src_ref=send_y.at[to], dst_ref=recv_y.at[y],
            send_sem=sem_y_s.at[i], recv_sem=sem_y_r.at[i],
            device_id={"tp": to * NX + x}, device_id_type=MESH,
        )

    for i in range(1, n_y):
        col_copy(i).start()
    recv_y[y] = send_y[y]

    def act_done():
        piece = acts.at[pl.ds(0, n_tp - 1)]
        done = plane(piece, piece, sem_act, lax.rem(me + 1, n_tp))
        done.wait_send()
        done.wait_recv()

    act_done()
    shared = tn(acts[...].reshape(n_tp * per_j, tokens), sdown[...])
    mixed = halves(shared[:half], shared[half:])[0]
    for i in range(1, n_y):
        col_copy(i).wait_send()
        col_copy(i).wait_recv()
    for i in range(n_y):
        mixed += recv_y[i].astype(F32)
    mixed = mixed.T
    o_mix[...] = jnp.concatenate([mixed[:64], mixed[64:]], axis=1).astype(BF16)

    for d in (0, 1):
        for q in range(CHUNKS):

            def sent(s, _, d=d, q=q):
                hop(d, s, q, z).wait_send()
                return 0

            lax.fori_loop(1, far + (1 if last_leg(d, q) else 0), sent, 0)

        def small_sent(s, _, d=d):
            small_hop(d, s, z).wait_send()
            return 0

        lax.fori_loop(1, far + (1 if d == 0 else 0), small_sent, 0)

    def pair_sent(i, _):
        pair(i).wait_send()
        return 0

    lax.fori_loop(0, nz, pair_sent, 0)


def deliver(*refs):
    n = (len(refs) - 1) // 2
    copies = [pltpu.make_async_copy(refs[i], refs[n + i], refs[-1].at[i]) for i in range(n)]
    for copy in copies:
        copy.start()
    for copy in copies:
        copy.wait()


def on_device(*args):
    n_tp, units = args[0].shape[:2]
    nz = lax.axis_size("fs") // 2
    tokens, width = args[7].shape
    top = args[8].shape[1]
    cap = min(tokens, 5 * tokens * top // (2 * n_tp))
    hidden = nz * 2 * units
    per_j = -(-hidden // (16 * n_tp)) * 16
    n_y = n_tp // NX
    far = nz // 2
    groups = nz // 4
    args = [jnp.swapaxes(v, 0, 1) for v in args[:3]] + list(args[3:])
    args[6] = args[6].reshape(1, -1)
    args[8:] = [v.T for v in args[8:]]
    vm = pl.BlockSpec(memory_space=pltpu.VMEM)
    hbm = pl.BlockSpec(memory_space=pl.ANY)
    dma = pltpu.SemaphoreType.DMA
    big = pltpu.VMEM((groups, 8 * units, width), BF16)
    thin = pltpu.VMEM((64, hidden), BF16)
    mix = pltpu.VMEM((64, tokens), BF16)
    outs = pl.pallas_call(
        functools.partial(kernel, n_tp, nz, units, cap),
        name="hand_over",
        out_shape=[big, big, big, thin, thin, thin, mix],
        in_specs=[vm] * 10,
        out_specs=[vm] * 7,
        scratch_shapes=[
            pltpu.VMEM((n_tp, ROW // 2, 128), F32),
            pltpu.VMEM((n_tp, ROW // 2, 128), BF16),
            pltpu.VMEM((n_tp, ROW // 2, 128), BF16),
            pltpu.VMEM((nz, 2, ROW, width), BF16),
            pltpu.VMEM((nz, 2, ROW // 2, 128), BF16),
            pltpu.VMEM((tokens, width), BF16),
            pltpu.VMEM((cap, width), BF16),
            pltpu.VMEM((cap, width), F32),
            pltpu.VMEM((NX, tokens, cap), BF16),
            pltpu.VMEM((cap, 128), F32),
            pltpu.VMEM((n_tp, per_j, 128), BF16),
            pltpu.VMEM((n_tp, per_j, 128), BF16),
            pltpu.VMEM((n_tp, per_j, tokens), BF16),
            pltpu.VMEM((n_tp * per_j, 128), BF16),
            pltpu.VMEM((NX, cap, 64 * n_y), BF16),
            pltpu.VMEM((NX, cap, 64 * n_y), BF16),
            pltpu.VMEM((n_y, tokens // 2, 128), BF16),
            pltpu.VMEM((n_y, tokens // 2, 128), BF16),
            dma((2,)),
            dma((2, far + 1, CHUNKS)),
            dma((2, far + 1, CHUNKS)),
            dma((nz,)),
            dma((nz,)),
            dma((2, far + 1)),
            dma((2, far + 1)),
            dma((2,)),
            dma((2,)),
            dma((2,)),
            dma((NX,)),
            dma((NX,)),
            dma((n_y,)),
            dma((n_y,)),
        ],
        compiler_params=pltpu.CompilerParams(
            collective_id=0, has_side_effects=True, vmem_limit_bytes=56 * 1024 * 1024
        ),
    )(*args)
    outs = pl.pallas_call(
        deliver,
        name="deliver",
        out_shape=[jax.ShapeDtypeStruct(v.shape, v.dtype) for v in outs],
        in_specs=[vm] * 7,
        out_specs=[hbm] * 7,
        scratch_shapes=[dma((7,))],
        compiler_params=pltpu.CompilerParams(vmem_limit_bytes=1024 * 1024),
    )(*[pltpu.with_memory_space_constraint(v, pltpu.VMEM) for v in outs])
    full = [v.reshape(1, hidden, width) for v in outs[:3]]
    return (*full, *[v.T for v in outs[3:]])


def solution(mesh):
    placed = (
        P(None, "fs", "tp"),
        P(None, "fs", "tp"),
        P(None, "fs", "tp"),
        P("fs", "tp"),
        P("fs", "tp"),
        P("fs", "tp"),
        P("tp"),
        P("fs", None),
        P("fs", None),
        P("fs", None),
    )
    return jax.shard_map(
        on_device,
        mesh=mesh,
        in_specs=placed,
        out_specs=(
            P("tp", None, None),
            P("tp", None, None),
            P("tp", None, None),
            P(None, "tp"),
            P(None, "tp"),
            P(None, "tp"),
            P("fs", "tp"),
        ),
        check_vma=False,
    )
```

```python
import functools

import jax
import jax.numpy as jnp
from jax import lax
from jax.experimental import pallas as pl
from jax.experimental.pallas import tpu as pltpu
from jax.sharding import PartitionSpec as P

EPSILON = 1e-06
ROUTED_SCALE = 2.5
MESH = pl.DeviceIdType.MESH
NX = 4
ROW = 64
PIECE = 16
ORDER = (0, 2, 1, 3)
F32, BF16 = jnp.float32, jnp.bfloat16


def nt(a, b):
    return lax.dot_general(a, b, (((1,), (1,)), ((), ())), preferred_element_type=F32)


def tn(a, b):
    return lax.dot_general(a, b, (((0,), (0,)), ((), ())), preferred_element_type=F32)


def nn(a, b):
    return jnp.dot(a, b, preferred_element_type=F32)


def iota(shape, dim):
    return lax.broadcasted_iota(jnp.int32, shape, dim)


def silu(v):
    return v / (1.0 + jnp.exp(-v))


def halves(a, b):
    low = iota(a.shape, len(a.shape) - 1) < 64
    ax = len(a.shape) - 1
    return (
        jnp.where(low, a, pltpu.roll(b, 64, ax)),
        jnp.where(low, pltpu.roll(a, 64, ax), b),
    )


def kernel(
    n_tp, nz, units, cap,
    *refs,
):
    hbm_in, refs = refs[:10], refs[10:]
    outs, refs = refs[:7], refs[7:]
    inputs, refs = refs[:10], refs[10:]
    body(n_tp, nz, units, cap, hbm_in, *inputs, *outs, *refs)


def body(
    n_tp, nz, units, cap, hbm_in,
    tg, tu, td, sg, su, sd, gain, tok, ids, scores,
    o_gate, o_up, o_down, o_sgate, o_sup, o_sdown, o_mix,
    packed, pick, send_a, recv_a, blocks, small, normed, rows, total, spread, slot_weight,
    pre_send, pre_recv, acts, sdown, send_x, recv_x, send_y, recv_y,
    sem_in, sem_a, sem_ring_s, sem_ring_r, sem_pair_s, sem_pair_r,
    sem_small_s, sem_small_r, sem_spair, sem_j, sem_act, sem_x_s, sem_x_r, sem_y_s, sem_y_r,
):
    n_y = n_tp // NX
    far = nz // 2
    groups = nz // 4
    group_rows = 8 * units
    hidden = nz * 2 * units
    per_j = pre_send.shape[1]
    width = total.shape[1]
    tokens = tok.shape[0]
    me = lax.axis_index("tp")
    fs = lax.axis_index("fs")
    z, core = fs // 2, lax.rem(fs, 2)
    y, x = me // NX, lax.rem(me, NX)
    ahead = lax.rem(z + 1, nz) * 2 + core
    behind = lax.rem(z + nz - 1, nz) * 2 + core
    twin = z * 2 + 1 - core

    barrier = pltpu.get_barrier_semaphore()

    def greet(i, _):
        peer = lax.rem(me + i, n_tp)
        pl.semaphore_signal(barrier, inc=1, device_id={"tp": peer}, device_id_type=MESH)
        return 0

    for other in (ahead, behind, twin):
        pl.semaphore_signal(barrier, inc=1, device_id={"fs": other}, device_id_type=MESH)
    lax.fori_loop(1, n_tp, greet, 0)
    vmem_in = (tg, tu, td, sg, su, sd, gain, tok, ids, scores)
    loads = [pltpu.make_async_copy(hbm_in[i], vmem_in[i], sem_in.at[i]) for i in range(10)]
    for load in loads:
        load.start()
    for i in (0, 1, 2, 3, 4, 5, 6):
        loads[i].wait()

    scale = gain[...]

    with jax.named_scope("pack"):

        def unit(r):
            if r < units:
                return tg[r] * scale
            if r < 2 * units:
                return tu[r - units] * scale
            return td[r - 2 * units] if r < 3 * units else jnp.zeros((n_tp, 64), F32)

        parts = [sg[...] * scale, su[...] * scale, sd[...]]
        stack = jnp.concatenate([*parts, jnp.zeros((ROW - 3 * units, 64), F32)], axis=0)
        stack = jnp.concatenate([stack[: ROW // 2], stack[ROW // 2 :]], axis=1)
        small[z, core] = stack.astype(BF16)
        for r in range(0, ROW // 2, 8):
            several = [
                jnp.concatenate([unit(i), unit(i + ROW // 2)], axis=1) for i in range(r, r + 8)
            ]
            packed[:, pl.ds(r, 8), :] = jnp.swapaxes(jnp.stack(several, axis=0), 0, 1)
        for h in (0, 1):
            send_a[h] = packed[:, pl.ds(PIECE * h, PIECE), :].astype(BF16)
            recv_a[h, me] = send_a[h, me]
    with jax.named_scope("entry"):
        pl.semaphore_wait(barrier, n_tp + 2)

    def plane(src, dst, sems, peer, at=0):
        return pltpu.make_async_remote_copy(
            src_ref=src, dst_ref=dst, send_sem=sems.at[at], recv_sem=sems.at[at + 1],
            device_id={"tp": peer}, device_id_type=MESH,
        )

    def plane_done(ref, sems, at=0):
        piece = ref.at[pl.ds(0, n_tp - 1)]
        done = plane(piece, piece, sems, lax.rem(me + 1, n_tp), at)
        done.wait_send()
        done.wait_recv()

    def small_hop(d, s, at):
        return pltpu.make_async_remote_copy(
            src_ref=small.at[at, core], dst_ref=small.at[at, core],
            send_sem=sem_small_s.at[d, s], recv_sem=sem_small_r.at[d, s],
            device_id={"fs": ahead if d == 0 else behind}, device_id_type=MESH,
        )

    def small_pair(at):
        return pltpu.make_async_remote_copy(
            src_ref=small.at[at, core], dst_ref=small.at[at, core],
            send_sem=sem_spair.at[0], recv_sem=sem_spair.at[1],
            device_id={"fs": twin}, device_id_type=MESH,
        )

    def origin(d, s):
        return lax.rem(z + nz - s, nz) if d == 0 else lax.rem(z + s, nz)

    small_hop(0, 1, z).start()
    small_hop(1, 1, z).start()
    small_pair(z).start()

    for h in (0, 1):

        def send_weights(i, _, h=h):
            peer = lax.rem(me + i, n_tp)
            plane(send_a.at[h, peer], recv_a.at[h, me], sem_a, peer, 2 * h).start()
            return 0

        lax.fori_loop(1, n_tp, send_weights, 0)

    def small_step(s):
        for d in (0, 1):

            def arrived(d=d):
                at = origin(d, s)
                small_hop(d, s, at).wait_recv()
                small_pair(at).start()

                @pl.when((s + 1 < far) | ((s + 1 == far) & (d == 0)))
                def _():
                    small_hop(d, s + 1, at).start()

            if d == 0:
                arrived()
            else:
                pl.when(s < far)(arrived)

    for i in (7, 8, 9):
        loads[i].wait()
    tf = tok[...].astype(F32)
    normed[...] = (
        tf * lax.rsqrt(jnp.mean(tf * tf, axis=1, keepdims=True) + EPSILON)
    ).astype(BF16)
    ids_v, sc = ids[...], scores[...]
    ratio = ROUTED_SCALE * sc / jnp.sum(sc, axis=0, keepdims=True)
    expert_row = iota((128, tokens), 0)
    present = jnp.zeros((128, tokens), F32)
    weight_row = jnp.zeros((1, tokens), F32)
    for k in range(ids.shape[0]):
        present = jnp.where(ids_v[k : k + 1] == expert_row, 1.0, present)
        weight_row += jnp.where(ids_v[k : k + 1] == me, ratio[k : k + 1], 0.0)
    before = jnp.where(iota((tokens, tokens), 0) < iota((tokens, tokens), 1), 1.0, 0.0)
    position = nn(present.astype(BF16), before.astype(BF16))
    slots = jnp.where(present > 0.0, position, -1.0)
    slot_row = jnp.sum(jnp.where(expert_row == me, slots, 0.0), axis=0, keepdims=True)
    slot = slots.T
    lane = iota((tokens, 128), 1)
    taken = slot_row == iota((cap, tokens), 0).astype(F32)
    slot_weight[...] = jnp.broadcast_to(
        jnp.sum(jnp.where(taken, weight_row, 0.0), axis=1, keepdims=True), slot_weight.shape
    )
    rows[...] = nn(jnp.where(taken, 1.0, 0.0).astype(BF16), normed[...]).astype(BF16)
    for i in range(NX):
        col = jnp.sum(jnp.where(lane == y * NX + i, slot, 0.0), axis=1, keepdims=True)
        spread[i] = jnp.where(col == iota((tokens, cap), 1).astype(F32), 1.0, 0.0).astype(BF16)
    total[...] = jnp.zeros_like(total)

    shape = (group_rows, 8 * ROW)
    i, f, r = iota(shape, 0), iota(shape, 1) // ROW, iota(shape, 1) & (ROW - 1)
    ordered = []
    for m in range(3):
        inside = (r >= units * m) & (r < units * (m + 1))
        ordered.append(jnp.where(inside & (i == units * f + r - units * m), 1.0, 0.0))
    pick[...] = jnp.concatenate(ordered, axis=0).astype(BF16)

    def hop(d, s, q, at):
        piece = blocks.at[at, core, pl.ds(q * PIECE, PIECE)]
        return pltpu.make_async_remote_copy(
            src_ref=piece, dst_ref=piece,
            send_sem=sem_ring_s.at[d, s, q], recv_sem=sem_ring_r.at[d, s, q],
            device_id={"fs": ahead if d == 0 else behind}, device_id_type=MESH,
        )

    def pair(at):
        rel = lax.rem(at + nz - z, nz)
        return pltpu.make_async_remote_copy(
            src_ref=blocks.at[at, core], dst_ref=blocks.at[at, core],
            send_sem=sem_pair_s.at[rel], recv_sem=sem_pair_r.at[rel],
            device_id={"fs": twin}, device_id_type=MESH,
        )

    early = far // 2
    with jax.named_scope("small_early"):
        for i in range(1, early + 1):
            small_step(i)
    for h in (0, 1):
        with jax.named_scope(f"await_weights{h}"):
            plane_done(recv_a.at[h], sem_a, 2 * h)
        with jax.named_scope("unpack"):
            for m in range(n_tp // 2):
                upper, lower = recv_a[h, 2 * m].astype(F32), recv_a[h, 2 * m + 1].astype(F32)
                for part, v in enumerate(halves(upper, lower)):
                    at = pl.ds(PIECE * (h + 2 * part), PIECE)
                    blocks[z, core, at, pl.ds(128 * m, 128)] = v.astype(BF16)
        for q in ORDER[2 * h : 2 * h + 2]:
            for d in (0, 1):
                hop(d, 1, q, z).start()
    pair(z).start()

    def last_leg(d, q):
        return (q in ORDER[:2]) == (d == 0)

    def activated(at):
        with jax.named_scope("await_pair"):
            pair(at).wait_recv()
        pre = nt(rows[...], blocks[at].reshape(2 * ROW, width))
        act = silu(pltpu.roll(pre, 2 * units, 1)) * pltpu.roll(pre, units, 1)
        unit = iota(act.shape, 1) & (ROW - 1)
        return jnp.where((unit >= 2 * units) & (unit < 3 * units), act, 0.0).astype(BF16)

    def expert(at):
        act = activated(at)
        total[...] += nn(act, blocks[at].reshape(2 * ROW, width))

    def padded(v):
        spare = jnp.zeros((-hidden % 128, 128), F32)
        return jnp.concatenate([v, spare], axis=0)

    def shared_rows():
        got = [[], [], []]
        for g in range(groups):
            v = small[pl.ds(4 * g, 4)].reshape(8, ROW // 2, 128).astype(F32)
            v = jnp.concatenate([v, pltpu.roll(v, 64, 2)], axis=1).reshape(8 * ROW, 128)
            v = v.astype(BF16)
            found = nn(pick[...], v)
            for m in range(3):
                got[m].append(found[group_rows * m : group_rows * (m + 1)])
        gate, up, down = [jnp.concatenate(one, axis=0) for one in got]
        for o, v in ((o_sgate, gate), (o_sup, up), (o_sdown, down)):
            o[...] = padded(v).T[:64, :hidden].astype(BF16)
        pad = jnp.zeros((n_tp * per_j - hidden, 128), F32)
        both = jnp.concatenate([halves(gate, up)[0], pad], axis=0)
        pre_send[...] = both.astype(BF16).reshape(n_tp, per_j, 128)
        low = iota(down.shape, 1) < 64
        down = jnp.concatenate([jnp.where(low, down, 0.0), pad], axis=0)
        sdown[...] = down.astype(BF16)
        pre_recv[me] = pre_send[me]

        def send(i, _):
            peer = lax.rem(me + i, n_tp)
            plane(pre_send.at[peer], pre_recv.at[me], sem_j, peer).start()
            return 0

        lax.fori_loop(1, n_tp, send, 0)

    def shared_acts():
        with jax.named_scope("await_j"):
            plane_done(pre_recv, sem_j)
        gates, ups = [], []
        for m in range(n_tp // 2):
            g, u = halves(pre_recv[2 * m].astype(F32), pre_recv[2 * m + 1].astype(F32))
            gates.append(g.astype(BF16))
            ups.append(u.astype(BF16))
        gate = nt(jnp.concatenate(gates, axis=1), normed[...])
        up = nt(jnp.concatenate(ups, axis=1), normed[...])
        acts[me] = (silu(gate) * up).astype(BF16)

        def send_act(i, _):
            peer = lax.rem(me + i, n_tp)
            plane(acts.at[me], acts.at[me], sem_act, peer).start()
            return 0

        lax.fori_loop(1, n_tp, send_act, 0)

    def ring_step(s, _):
        for n, q in enumerate(ORDER):
            for d in (0, 1):
                at = origin(d, s)
                with jax.named_scope(f"arrive{d}{n}"):
                    hop(d, s, q, at).wait_recv()
                if last_leg(d, q):
                    hop(d, s + 1, q, at).start()
                else:

                    @pl.when(s + 1 < far)
                    def _(d=d, q=q, at=at):
                        hop(d, s + 1, q, at).start()

            if n == 1:
                with jax.named_scope("expert0"):
                    expert(origin(0, s - 1))
            if n == 2:

                @pl.when(s > 1)
                def _():
                    with jax.named_scope("expert1"):
                        expert(origin(1, s - 1))

        for d in (0, 1):
            pair(origin(d, s)).start()

        @pl.when(s + early <= far)
        def _():
            with jax.named_scope("small"):
                small_step(s + early)

        @pl.when(s == far - early)
        def _():
            everything = small.at[:, 0]
            done = pltpu.make_async_remote_copy(
                src_ref=everything, dst_ref=everything,
                send_sem=sem_spair.at[0], recv_sem=sem_spair.at[1],
                device_id={"fs": twin}, device_id_type=MESH,
            )
            done.wait_send()
            done.wait_recv()
            with jax.named_scope("shared_rows"):
                shared_rows()

        @pl.when(s == far - early + 1)
        def _():
            with jax.named_scope("shared_acts"):
                shared_acts()

        return 0

    lax.fori_loop(1, far, ring_step, 0)
    for d in (0, 1):
        with jax.named_scope("expert_near_last"):
            expert(origin(d, far - 1))
    opposite = lax.rem(z + far, nz)
    with jax.named_scope("arrive_last"):
        for q in ORDER:
            hop(0 if q in ORDER[:2] else 1, far, q, opposite).wait_recv()
    pair(opposite).start()
    with jax.named_scope("expert_last"):
        act = activated(opposite)

    w = slot_weight[...]
    pairs = n_y // 2
    turns = [(pairs // 2 + (i + 1) // 2 * (1 if i % 2 else -1)) % pairs for i in range(pairs)]
    turns = [i for i in turns if i] + [0]

    def quarter(k):
        return lax.rem(y // 2 + turns[k], pairs)

    def row_copy(k, i):
        to = lax.rem(x + i, NX)
        return pltpu.make_async_remote_copy(
            src_ref=send_x.at[to, k], dst_ref=recv_x.at[x, k],
            send_sem=sem_x_s.at[k, i], recv_sem=sem_x_r.at[k, i],
            device_id={"tp": y * NX + to}, device_id_type=MESH,
        )

    for k in range(pairs):
        p = quarter(k)
        for h in range(NX // 2):
            several = []
            for i in (2 * p, 2 * p + 1):
                cols = pl.ds(pl.multiple_of(128 * (i * (NX // 2) + h), 128), 128)
                new = nn(act, blocks[opposite, :, :, cols].reshape(2 * ROW, 128))
                several.append((total[:, cols] + new) * w)
            for i, v in enumerate(halves(*several)):
                send_x[2 * h + i, k] = v.astype(BF16)
        for i in (2, 1, 3) if NX == 4 else range(1, NX):
            row_copy(k, i).start()
        recv_x[x, k] = send_x[x, k]

    part = min(512, width)
    results = (o_gate, o_up, o_down)

    def served(g):
        def some(n, _):
            cols = pl.ds(pl.multiple_of(n * part, part), part)
            v = blocks[pl.ds(4 * g, 4), :, :, cols].reshape(8 * ROW, part)
            v = nn(pick[...], v)
            for m in range(3):
                results[m][g, :, cols] = v[group_rows * m : group_rows * (m + 1)].astype(BF16)
            return 0

        with jax.named_scope("served"):
            lax.fori_loop(0, width // part, some, 0)

    for g in range(groups - 1):
        served(g)

    half = tokens // 2
    odd = lax.rem(y, 2)

    def col_copy(k, h):
        last = k == pairs - 1
        to = 2 * quarter(k) + (1 - odd if last else h)
        return pltpu.make_async_remote_copy(
            src_ref=send_y.at[to], dst_ref=recv_y.at[y],
            send_sem=sem_y_s.at[k, h], recv_sem=sem_y_r.at[k, 0 if last else odd],
            device_id={"tp": to * NX + x}, device_id_type=MESH,
        )

    def col_arrival(k, h):
        return pltpu.make_async_remote_copy(
            src_ref=recv_y.at[0], dst_ref=recv_y.at[0],
            send_sem=sem_y_s.at[k, h], recv_sem=sem_y_r.at[k, h],
            device_id={"tp": lax.rem(me + 1, n_tp)}, device_id_type=MESH,
        )

    y_copies = [(k, h) for k in range(pairs) for h in (0, 1) if k < pairs - 1 or h == 0]
    for k in range(pairs):
        with jax.named_scope(f"await_x{k}"):
            for i in range(1, NX):
                row_copy(k, i).wait_recv()
        acc = jnp.zeros((tokens, 128), F32)
        for i in range(NX):
            acc += nn(spread[i], recv_x[i, k])
        for h, v in enumerate(halves(acc[:half], acc[half:])):
            send_y[2 * quarter(k) + h] = v.astype(BF16)
        for h in (0, 1):
            if (k, h) in y_copies:
                col_copy(k, h).start()
    recv_y[y] = send_y[y]
    served(groups - 1)

    with jax.named_scope("await_act"):
        plane_done(acts, sem_act)
    shared = tn(acts[...].reshape(n_tp * per_j, tokens), sdown[...])
    mixed = halves(shared[:half], shared[half:])[0]
    with jax.named_scope("await_y"):
        for k, h in y_copies:
            col_arrival(k, h).wait_recv()
    for i in range(n_y):
        mixed += recv_y[i].astype(F32)
    mixed = mixed.T
    o_mix[...] = jnp.concatenate([mixed[:64], mixed[64:]], axis=1).astype(BF16)

    for d in (0, 1):
        for q in ORDER:

            def sent(s, _, d=d, q=q):
                hop(d, s, q, z).wait_send()
                return 0

            lax.fori_loop(1, far + (1 if last_leg(d, q) else 0), sent, 0)

        def small_sent(s, _, d=d):
            small_hop(d, s, z).wait_send()
            return 0

        lax.fori_loop(1, far + (1 if d == 0 else 0), small_sent, 0)

    def pair_sent(i, _):
        pair(i).wait_send()
        return 0

    lax.fori_loop(0, nz, pair_sent, 0)
    for k in range(pairs):
        for i in range(1, NX):
            row_copy(k, i).wait_send()
    for k, h in y_copies:
        col_copy(k, h).wait_send()


def deliver(*refs):
    n = (len(refs) - 1) // 2
    copies = [pltpu.make_async_copy(refs[i], refs[n + i], refs[-1].at[i]) for i in range(n)]
    for copy in copies:
        copy.start()
    for copy in copies:
        copy.wait()


def on_device(*args):
    n_tp, units = args[0].shape[:2]
    nz = lax.axis_size("fs") // 2
    tokens, width = args[7].shape
    top = args[8].shape[1]
    cap = min(tokens, 5 * tokens * top // (2 * n_tp))
    hidden = nz * 2 * units
    per_j = -(-hidden // (16 * n_tp)) * 16
    n_y = n_tp // NX
    far = nz // 2
    groups = nz // 4
    args = [jnp.swapaxes(v, 0, 1) for v in args[:3]] + list(args[3:])
    args[6] = args[6].reshape(1, -1)
    args[8:] = [v.T for v in args[8:]]
    vm = pl.BlockSpec(memory_space=pltpu.VMEM)
    hbm = pl.BlockSpec(memory_space=pl.ANY)
    dma = pltpu.SemaphoreType.DMA
    big = pltpu.VMEM((groups, 8 * units, width), BF16)
    thin = pltpu.VMEM((64, hidden), BF16)
    mix = pltpu.VMEM((64, tokens), BF16)
    outs = pl.pallas_call(
        functools.partial(kernel, n_tp, nz, units, cap),
        name="hand_over",
        out_shape=[big, big, big, thin, thin, thin, mix],
        in_specs=[hbm] * 10,
        out_specs=[vm] * 7,
        scratch_shapes=[
            *[pltpu.VMEM(v.shape, v.dtype) for v in args],
            pltpu.VMEM((n_tp, ROW // 2, 128), F32),
            pltpu.VMEM((24 * units, 8 * ROW), BF16),
            pltpu.VMEM((2, n_tp, PIECE, 128), BF16),
            pltpu.VMEM((2, n_tp, PIECE, 128), BF16),
            pltpu.VMEM((nz, 2, ROW, width), BF16),
            pltpu.VMEM((nz, 2, ROW // 2, 128), BF16),
            pltpu.VMEM((tokens, width), BF16),
            pltpu.VMEM((cap, width), BF16),
            pltpu.VMEM((cap, width), F32),
            pltpu.VMEM((NX, tokens, cap), BF16),
            pltpu.VMEM((cap, 128), F32),
            pltpu.VMEM((n_tp, per_j, 128), BF16),
            pltpu.VMEM((n_tp, per_j, 128), BF16),
            pltpu.VMEM((n_tp, per_j, tokens), BF16),
            pltpu.VMEM((n_tp * per_j, 128), BF16),
            pltpu.VMEM((NX, n_y // 2, cap, 128), BF16),
            pltpu.VMEM((NX, n_y // 2, cap, 128), BF16),
            pltpu.VMEM((n_y, tokens // 2, 128), BF16),
            pltpu.VMEM((n_y, tokens // 2, 128), BF16),
            dma((10,)),
            dma((4,)),
            dma((2, far + 1, len(ORDER))),
            dma((2, far + 1, len(ORDER))),
            dma((nz,)),
            dma((nz,)),
            dma((2, far + 1)),
            dma((2, far + 1)),
            dma((2,)),
            dma((2,)),
            dma((2,)),
            dma((n_y // 2, NX)),
            dma((n_y // 2, NX)),
            dma((n_y // 2, 2)),
            dma((n_y // 2, 2)),
        ],
        compiler_params=pltpu.CompilerParams(
            collective_id=0, has_side_effects=True, vmem_limit_bytes=56 * 1024 * 1024
        ),
    )(*args)
    outs = pl.pallas_call(
        deliver,
        name="deliver",
        out_shape=[jax.ShapeDtypeStruct(v.shape, v.dtype) for v in outs],
        in_specs=[vm] * 7,
        out_specs=[hbm] * 7,
        scratch_shapes=[dma((7,))],
        compiler_params=pltpu.CompilerParams(vmem_limit_bytes=1024 * 1024),
    )(*[pltpu.with_memory_space_constraint(v, pltpu.VMEM) for v in outs])
    full = [v.reshape(1, hidden, width) for v in outs[:3]]
    return (*full, *[v.T for v in outs[3:]])


def solution(mesh):
    placed = (
        P(None, "fs", "tp"),
        P(None, "fs", "tp"),
        P(None, "fs", "tp"),
        P("fs", "tp"),
        P("fs", "tp"),
        P("fs", "tp"),
        P("tp"),
        P("fs", None),
        P("fs", None),
        P("fs", None),
    )
    return jax.shard_map(
        on_device,
        mesh=mesh,
        in_specs=placed,
        out_specs=(
            P("tp", None, None),
            P("tp", None, None),
            P("tp", None, None),
            P(None, "tp"),
            P(None, "tp"),
            P(None, "tp"),
            P("fs", "tp"),
        ),
        check_vma=False,
    )
```

```python
import functools

import jax
import jax.numpy as jnp
from jax import lax
from jax.experimental import pallas as pl
from jax.experimental.pallas import tpu as pltpu
from jax.sharding import PartitionSpec as P

EPSILON = 1e-06
ROUTED_SCALE = 2.5
MESH = pl.DeviceIdType.MESH
NX = 4
ROW = 64
PIECE = 16
ORDER = (0, 2, 1, 3)
F32, BF16 = jnp.float32, jnp.bfloat16


def nt(a, b):
    return lax.dot_general(a, b, (((1,), (1,)), ((), ())), preferred_element_type=F32)


def tn(a, b):
    return lax.dot_general(a, b, (((0,), (0,)), ((), ())), preferred_element_type=F32)


def nn(a, b):
    return jnp.dot(a, b, preferred_element_type=F32)


def iota(shape, dim):
    return lax.broadcasted_iota(jnp.int32, shape, dim)


def silu(v):
    return v / (1.0 + jnp.exp(-v))


def halves(a, b):
    low = iota(a.shape, len(a.shape) - 1) < 64
    ax = len(a.shape) - 1
    return (
        jnp.where(low, a, pltpu.roll(b, 64, ax)),
        jnp.where(low, pltpu.roll(a, 64, ax), b),
    )


def kernel(
    n_tp, nz, units, cap,
    *refs,
):
    hbm_in, refs = refs[:10], refs[10:]
    outs, refs = refs[:7], refs[7:]
    inputs, refs = refs[:10], refs[10:]
    body(n_tp, nz, units, cap, hbm_in, *inputs, *outs, *refs)


def body(
    n_tp, nz, units, cap, hbm_in,
    tg, tu, td, sg, su, sd, gain, tok, ids, scores,
    o_gate, o_up, o_down, o_sgate, o_sup, o_sdown, o_mix,
    packed, pick, send_a, recv_a, blocks, small, normed, rows, total, spread, slot_weight,
    pre_send, pre_recv, acts, sdown, send_x, recv_x, send_y, recv_y,
    sem_in, sem_a, sem_ring_s, sem_ring_r, sem_pair_s, sem_pair_r,
    sem_small_s, sem_small_r, sem_spair, sem_j, sem_act, sem_x_s, sem_x_r, sem_y_s, sem_y_r,
):
    n_y = n_tp // NX
    far = nz // 2
    groups = nz // 4
    group_rows = 8 * units
    hidden = nz * 2 * units
    per_j = pre_send.shape[1]
    width = total.shape[1]
    tokens = tok.shape[0]
    me = lax.axis_index("tp")
    fs = lax.axis_index("fs")
    z, core = fs // 2, lax.rem(fs, 2)
    y, x = me // NX, lax.rem(me, NX)
    ahead = lax.rem(z + 1, nz) * 2 + core
    behind = lax.rem(z + nz - 1, nz) * 2 + core
    twin = z * 2 + 1 - core

    barrier = pltpu.get_barrier_semaphore()

    def greet(i, _):
        peer = lax.rem(me + i, n_tp)
        pl.semaphore_signal(barrier, inc=1, device_id={"tp": peer}, device_id_type=MESH)
        return 0

    vmem_in = (tg, tu, td, sg, su, sd, gain, tok, ids, scores)
    loads = [pltpu.make_async_copy(hbm_in[i], vmem_in[i], sem_in.at[i]) for i in range(10)]
    for load in loads:
        load.start()
    for other in (ahead, behind, twin):
        pl.semaphore_signal(barrier, inc=1, device_id={"fs": other}, device_id_type=MESH)
    lax.fori_loop(1, n_tp, greet, 0)
    for i in (0, 1, 2, 3, 4, 5, 6):
        loads[i].wait()

    scale = gain[...]

    with jax.named_scope("pack"):

        def unit(r):
            if r < units:
                return tg[r] * scale
            if r < 2 * units:
                return tu[r - units] * scale
            return td[r - 2 * units] if r < 3 * units else jnp.zeros((n_tp, 64), F32)

        parts = [sg[...] * scale, su[...] * scale, sd[...]]
        stack = jnp.concatenate([*parts, jnp.zeros((ROW - 3 * units, 64), F32)], axis=0)
        stack = jnp.concatenate([stack[: ROW // 2], stack[ROW // 2 :]], axis=1)
        small[z, core] = stack.astype(BF16)
        for r in range(0, ROW // 2, 8):
            several = [
                jnp.concatenate([unit(i), unit(i + ROW // 2)], axis=1) for i in range(r, r + 8)
            ]
            packed[:, pl.ds(r, 8), :] = jnp.swapaxes(jnp.stack(several, axis=0), 0, 1)
        for h in (0, 1):
            send_a[h] = packed[:, pl.ds(PIECE * h, PIECE), :].astype(BF16)
            recv_a[h, me] = send_a[h, me]
    with jax.named_scope("entry"):
        pl.semaphore_wait(barrier, n_tp + 2)

    def plane(src, dst, sems, peer, at=0):
        return pltpu.make_async_remote_copy(
            src_ref=src, dst_ref=dst, send_sem=sems.at[at], recv_sem=sems.at[at + 1],
            device_id={"tp": peer}, device_id_type=MESH,
        )

    def plane_done(ref, sems, at=0):
        piece = ref.at[pl.ds(0, n_tp - 1)]
        done = plane(piece, piece, sems, lax.rem(me + 1, n_tp), at)
        done.wait_send()
        done.wait_recv()

    def small_hop(d, s, at):
        return pltpu.make_async_remote_copy(
            src_ref=small.at[at, core], dst_ref=small.at[at, core],
            send_sem=sem_small_s.at[d, s], recv_sem=sem_small_r.at[d, s],
            device_id={"fs": ahead if d == 0 else behind}, device_id_type=MESH,
        )

    def small_pair(at):
        return pltpu.make_async_remote_copy(
            src_ref=small.at[at, core], dst_ref=small.at[at, core],
            send_sem=sem_spair.at[0], recv_sem=sem_spair.at[1],
            device_id={"fs": twin}, device_id_type=MESH,
        )

    def origin(d, s):
        return lax.rem(z + nz - s, nz) if d == 0 else lax.rem(z + s, nz)

    small_hop(0, 1, z).start()
    small_hop(1, 1, z).start()
    small_pair(z).start()

    away = [(min(i, n_y - i) + min(j, NX - j), i, j) for i in range(n_y) for j in range(NX)]
    for h in (0, 1):
        for distance, i, j in sorted(away, reverse=True):
            if distance:
                peer = lax.rem(y + i, n_y) * NX + lax.rem(x + j, NX)
                plane(send_a.at[h, peer], recv_a.at[h, me], sem_a, peer, 2 * h).start()

    def small_step(s):
        for d in (0, 1):

            def arrived(d=d):
                at = origin(d, s)
                small_hop(d, s, at).wait_recv()
                small_pair(at).start()

                @pl.when((s + 1 < far) | ((s + 1 == far) & (d == 0)))
                def _():
                    small_hop(d, s + 1, at).start()

            if d == 0:
                arrived()
            else:
                pl.when(s < far)(arrived)

    for i in (7, 8, 9):
        loads[i].wait()
    tf = tok[...].astype(F32)
    normed[...] = (
        tf * lax.rsqrt(jnp.mean(tf * tf, axis=1, keepdims=True) + EPSILON)
    ).astype(BF16)
    ids_v, sc = ids[...], scores[...]
    ratio = ROUTED_SCALE * sc / jnp.sum(sc, axis=0, keepdims=True)
    expert_row = iota((128, tokens), 0)
    present = jnp.zeros((128, tokens), F32)
    weight_row = jnp.zeros((1, tokens), F32)
    for k in range(ids.shape[0]):
        present = jnp.where(ids_v[k : k + 1] == expert_row, 1.0, present)
        weight_row += jnp.where(ids_v[k : k + 1] == me, ratio[k : k + 1], 0.0)
    before = jnp.where(iota((tokens, tokens), 0) < iota((tokens, tokens), 1), 1.0, 0.0)
    position = nn(present.astype(BF16), before.astype(BF16))
    slots = jnp.where(present > 0.0, position, -1.0)
    slot_row = jnp.sum(jnp.where(expert_row == me, slots, 0.0), axis=0, keepdims=True)
    slot = slots.T
    lane = iota((tokens, 128), 1)
    taken = slot_row == iota((cap, tokens), 0).astype(F32)
    slot_weight[...] = jnp.broadcast_to(
        jnp.sum(jnp.where(taken, weight_row, 0.0), axis=1, keepdims=True), slot_weight.shape
    )
    rows[...] = nn(jnp.where(taken, 1.0, 0.0).astype(BF16), normed[...]).astype(BF16)
    for i in range(NX):
        col = jnp.sum(jnp.where(lane == y * NX + i, slot, 0.0), axis=1, keepdims=True)
        spread[i] = jnp.where(col == iota((tokens, cap), 1).astype(F32), 1.0, 0.0).astype(BF16)
    total[...] = jnp.zeros_like(total)

    shape = (group_rows, 8 * ROW)
    i, f, r = iota(shape, 0), iota(shape, 1) // ROW, iota(shape, 1) & (ROW - 1)
    ordered = []
    for m in range(3):
        inside = (r >= units * m) & (r < units * (m + 1))
        ordered.append(jnp.where(inside & (i == units * f + r - units * m), 1.0, 0.0))
    pick[...] = jnp.concatenate(ordered, axis=0).astype(BF16)

    def hop(d, s, q, at):
        piece = blocks.at[at, core, pl.ds(q * PIECE, PIECE)]
        return pltpu.make_async_remote_copy(
            src_ref=piece, dst_ref=piece,
            send_sem=sem_ring_s.at[d, s, q], recv_sem=sem_ring_r.at[d, s, q],
            device_id={"fs": ahead if d == 0 else behind}, device_id_type=MESH,
        )

    def pair(at):
        rel = lax.rem(at + nz - z, nz)
        return pltpu.make_async_remote_copy(
            src_ref=blocks.at[at, core], dst_ref=blocks.at[at, core],
            send_sem=sem_pair_s.at[rel], recv_sem=sem_pair_r.at[rel],
            device_id={"fs": twin}, device_id_type=MESH,
        )

    early = 2
    with jax.named_scope("small_early"):
        for i in range(1, early + 1):
            small_step(i)
    for h in (0, 1):
        with jax.named_scope(f"await_weights{h}"):
            plane_done(recv_a.at[h], sem_a, 2 * h)
        with jax.named_scope("unpack"):
            for m in range(n_tp // 2):
                upper, lower = recv_a[h, 2 * m].astype(F32), recv_a[h, 2 * m + 1].astype(F32)
                for part, v in enumerate(halves(upper, lower)):
                    at = pl.ds(PIECE * (h + 2 * part), PIECE)
                    blocks[z, core, at, pl.ds(128 * m, 128)] = v.astype(BF16)
        for q in ORDER[2 * h : 2 * h + 2]:
            for d in (0, 1):
                hop(d, 1, q, z).start()
    pair(z).start()

    def last_leg(d, q):
        return (q in ORDER[:2]) == (d == 0)

    def activated(at):
        with jax.named_scope("await_pair"):
            pair(at).wait_recv()
        pre = nt(rows[...], blocks[at].reshape(2 * ROW, width))
        act = silu(pltpu.roll(pre, 2 * units, 1)) * pltpu.roll(pre, units, 1)
        unit = iota(act.shape, 1) & (ROW - 1)
        return jnp.where((unit >= 2 * units) & (unit < 3 * units), act, 0.0).astype(BF16)

    def expert(at):
        act = activated(at)
        total[...] += nn(act, blocks[at].reshape(2 * ROW, width))

    def padded(v):
        spare = jnp.zeros((-hidden % 128, 128), F32)
        return jnp.concatenate([v, spare], axis=0)

    def shared_rows():
        got = [[], [], []]
        for g in range(groups):
            v = small[pl.ds(4 * g, 4)].reshape(8, ROW // 2, 128).astype(F32)
            v = jnp.concatenate([v, pltpu.roll(v, 64, 2)], axis=1).reshape(8 * ROW, 128)
            v = v.astype(BF16)
            found = nn(pick[...], v)
            for m in range(3):
                got[m].append(found[group_rows * m : group_rows * (m + 1)])
        gate, up, down = [jnp.concatenate(one, axis=0) for one in got]
        for o, v in ((o_sgate, gate), (o_sup, up), (o_sdown, down)):
            o[...] = padded(v).T[:64, :hidden].astype(BF16)
        pad = jnp.zeros((n_tp * per_j - hidden, 128), F32)
        both = jnp.concatenate([halves(gate, up)[0], pad], axis=0)
        pre_send[...] = both.astype(BF16).reshape(n_tp, per_j, 128)
        low = iota(down.shape, 1) < 64
        down = jnp.concatenate([jnp.where(low, down, 0.0), pad], axis=0)
        sdown[...] = down.astype(BF16)
        pre_recv[me] = pre_send[me]

        def send(i, _):
            peer = lax.rem(me + i, n_tp)
            plane(pre_send.at[peer], pre_recv.at[me], sem_j, peer).start()
            return 0

        lax.fori_loop(1, n_tp, send, 0)

    def shared_acts():
        with jax.named_scope("await_j"):
            plane_done(pre_recv, sem_j)
        gates, ups = [], []
        for m in range(n_tp // 2):
            g, u = halves(pre_recv[2 * m].astype(F32), pre_recv[2 * m + 1].astype(F32))
            gates.append(g.astype(BF16))
            ups.append(u.astype(BF16))
        gate = nt(jnp.concatenate(gates, axis=1), normed[...])
        up = nt(jnp.concatenate(ups, axis=1), normed[...])
        acts[me] = (silu(gate) * up).astype(BF16)

        def send_act(i, _):
            peer = lax.rem(me + i, n_tp)
            plane(acts.at[me], acts.at[me], sem_act, peer).start()
            return 0

        lax.fori_loop(1, n_tp, send_act, 0)

    def ring_step(s, _):
        for n, q in enumerate(ORDER):
            for d in (0, 1):
                at = origin(d, s)
                with jax.named_scope(f"arrive{d}{n}"):
                    hop(d, s, q, at).wait_recv()
                if last_leg(d, q):
                    hop(d, s + 1, q, at).start()
                else:

                    @pl.when(s + 1 < far)
                    def _(d=d, q=q, at=at):
                        hop(d, s + 1, q, at).start()

            if 0 < n < 3:

                @pl.when(s == far - 1)
                def _(d=n - 1):
                    with jax.named_scope(f"expert_in{d}"):
                        expert(origin(d, s - 1))

        for d in (0, 1):
            pair(origin(d, s)).start()

        @pl.when(s + early <= far)
        def _():
            with jax.named_scope("small"):
                small_step(s + early)

        def one(i, _):
            with jax.named_scope("expert"):
                expert(lax.rem(z + nz + (s - 1) * (1 - 2 * i), nz))
            return 0

        @pl.when(s < far - 1)
        def _():
            lax.fori_loop(0, jnp.where(s == 1, 1, 2), one, 0)

        return 0

    lax.fori_loop(1, far, ring_step, 0)
    with jax.named_scope("await_small"):
        everything = small.at[:, 0]
        done = pltpu.make_async_remote_copy(
            src_ref=everything, dst_ref=everything,
            send_sem=sem_spair.at[0], recv_sem=sem_spair.at[1],
            device_id={"fs": twin}, device_id_type=MESH,
        )
        done.wait_send()
        done.wait_recv()
    with jax.named_scope("shared_rows"):
        shared_rows()
    opposite = lax.rem(z + far, nz)
    for d in (0, 1):
        with jax.named_scope(f"expert_near{d}"):
            expert(origin(d, far - 1))
        if d == 0:
            with jax.named_scope("arrive_last"):
                for q in ORDER:
                    hop(0 if q in ORDER[:2] else 1, far, q, opposite).wait_recv()
            pair(opposite).start()
    with jax.named_scope("expert_last"):
        act = activated(opposite)

    w = slot_weight[...]
    pairs = n_y // 2
    turns = [(pairs // 2 + (i + 1) // 2 * (1 if i % 2 else -1)) % pairs for i in range(pairs)]
    turns = [i for i in turns if i] + [0]

    def quarter(k):
        return lax.rem(y // 2 + turns[k], pairs)

    def row_copy(k, i):
        to = lax.rem(x + i, NX)
        return pltpu.make_async_remote_copy(
            src_ref=send_x.at[to, k], dst_ref=recv_x.at[x, k],
            send_sem=sem_x_s.at[k, i], recv_sem=sem_x_r.at[k, i],
            device_id={"tp": y * NX + to}, device_id_type=MESH,
        )

    for k in range(pairs):
        p = quarter(k)
        for h in range(NX // 2):
            several = []
            for i in (2 * p, 2 * p + 1):
                cols = pl.ds(pl.multiple_of(128 * (i * (NX // 2) + h), 128), 128)
                new = nn(act, blocks[opposite, :, :, cols].reshape(2 * ROW, 128))
                several.append((total[:, cols] + new) * w)
            for i, v in enumerate(halves(*several)):
                send_x[2 * h + i, k] = v.astype(BF16)
        for i in (2, 1, 3) if NX == 4 else range(1, NX):
            row_copy(k, i).start()
        recv_x[x, k] = send_x[x, k]

    part = min(512, width)
    results = (o_gate, o_up, o_down)

    def served(g):
        def some(n, _):
            cols = pl.ds(pl.multiple_of(n * part, part), part)
            v = blocks[pl.ds(4 * g, 4), :, :, cols].reshape(8 * ROW, part)
            v = nn(pick[...], v)
            for m in range(3):
                results[m][g, :, cols] = v[group_rows * m : group_rows * (m + 1)].astype(BF16)
            return 0

        with jax.named_scope("served"):
            lax.fori_loop(0, width // part, some, 0)

    served(0)
    with jax.named_scope("shared_acts"):
        shared_acts()
    for g in range(1, groups - 1):
        served(g)

    half = tokens // 2
    odd = lax.rem(y, 2)

    def col_copy(k, h):
        last = k == pairs - 1
        to = 2 * quarter(k) + (1 - odd if last else h)
        return pltpu.make_async_remote_copy(
            src_ref=send_y.at[to], dst_ref=recv_y.at[y],
            send_sem=sem_y_s.at[k, h], recv_sem=sem_y_r.at[k, 0 if last else odd],
            device_id={"tp": to * NX + x}, device_id_type=MESH,
        )

    def col_arrival(k, h):
        return pltpu.make_async_remote_copy(
            src_ref=recv_y.at[0], dst_ref=recv_y.at[0],
            send_sem=sem_y_s.at[k, h], recv_sem=sem_y_r.at[k, h],
            device_id={"tp": lax.rem(me + 1, n_tp)}, device_id_type=MESH,
        )

    y_copies = [(k, h) for k in range(pairs) for h in (0, 1) if k < pairs - 1 or h == 0]
    for k in range(pairs):
        with jax.named_scope(f"await_x{k}"):
            for i in range(1, NX):
                row_copy(k, i).wait_recv()
        acc = jnp.zeros((tokens, 128), F32)
        for i in range(NX):
            acc += nn(spread[i], recv_x[i, k])
        for h, v in enumerate(halves(acc[:half], acc[half:])):
            send_y[2 * quarter(k) + h] = v.astype(BF16)
        for h in (0, 1):
            if (k, h) in y_copies:
                col_copy(k, h).start()
    recv_y[y] = send_y[y]
    served(groups - 1)

    with jax.named_scope("await_act"):
        plane_done(acts, sem_act)
    shared = tn(acts[...].reshape(n_tp * per_j, tokens), sdown[...])
    mixed = halves(shared[:half], shared[half:])[0]
    with jax.named_scope("await_y"):
        for k, h in y_copies:
            col_arrival(k, h).wait_recv()
    for i in range(n_y):
        mixed += recv_y[i].astype(F32)
    mixed = mixed.T
    o_mix[...] = jnp.concatenate([mixed[:64], mixed[64:]], axis=1).astype(BF16)

    for d in (0, 1):
        for q in ORDER:

            def sent(s, _, d=d, q=q):
                hop(d, s, q, z).wait_send()
                return 0

            lax.fori_loop(1, far + (1 if last_leg(d, q) else 0), sent, 0)

        def small_sent(s, _, d=d):
            small_hop(d, s, z).wait_send()
            return 0

        lax.fori_loop(1, far + (1 if d == 0 else 0), small_sent, 0)

    def pair_sent(i, _):
        pair(i).wait_send()
        return 0

    lax.fori_loop(0, nz, pair_sent, 0)
    for k in range(pairs):
        for i in range(1, NX):
            row_copy(k, i).wait_send()
    for k, h in y_copies:
        col_copy(k, h).wait_send()


def deliver(*refs):
    n = (len(refs) - 1) // 2
    copies = [pltpu.make_async_copy(refs[i], refs[n + i], refs[-1].at[i]) for i in range(n)]
    for copy in copies:
        copy.start()
    for copy in copies:
        copy.wait()


def on_device(*args):
    n_tp, units = args[0].shape[:2]
    nz = lax.axis_size("fs") // 2
    tokens, width = args[7].shape
    top = args[8].shape[1]
    cap = min(tokens, 5 * tokens * top // (2 * n_tp))
    hidden = nz * 2 * units
    per_j = -(-hidden // (16 * n_tp)) * 16
    n_y = n_tp // NX
    far = nz // 2
    groups = nz // 4
    args = [jnp.swapaxes(v, 0, 1) for v in args[:3]] + list(args[3:])
    args[6] = args[6].reshape(1, -1)
    args[8:] = [v.T for v in args[8:]]
    vm = pl.BlockSpec(memory_space=pltpu.VMEM)
    hbm = pl.BlockSpec(memory_space=pl.ANY)
    dma = pltpu.SemaphoreType.DMA
    big = pltpu.VMEM((groups, 8 * units, width), BF16)
    thin = pltpu.VMEM((64, hidden), BF16)
    mix = pltpu.VMEM((64, tokens), BF16)
    outs = pl.pallas_call(
        functools.partial(kernel, n_tp, nz, units, cap),
        name="hand_over",
        out_shape=[big, big, big, thin, thin, thin, mix],
        in_specs=[hbm] * 10,
        out_specs=[vm] * 7,
        scratch_shapes=[
            *[pltpu.VMEM(v.shape, v.dtype) for v in args],
            pltpu.VMEM((n_tp, ROW // 2, 128), F32),
            pltpu.VMEM((24 * units, 8 * ROW), BF16),
            pltpu.VMEM((2, n_tp, PIECE, 128), BF16),
            pltpu.VMEM((2, n_tp, PIECE, 128), BF16),
            pltpu.VMEM((nz, 2, ROW, width), BF16),
            pltpu.VMEM((nz, 2, ROW // 2, 128), BF16),
            pltpu.VMEM((tokens, width), BF16),
            pltpu.VMEM((cap, width), BF16),
            pltpu.VMEM((cap, width), F32),
            pltpu.VMEM((NX, tokens, cap), BF16),
            pltpu.VMEM((cap, 128), F32),
            pltpu.VMEM((n_tp, per_j, 128), BF16),
            pltpu.VMEM((n_tp, per_j, 128), BF16),
            pltpu.VMEM((n_tp, per_j, tokens), BF16),
            pltpu.VMEM((n_tp * per_j, 128), BF16),
            pltpu.VMEM((NX, n_y // 2, cap, 128), BF16),
            pltpu.VMEM((NX, n_y // 2, cap, 128), BF16),
            pltpu.VMEM((n_y, tokens // 2, 128), BF16),
            pltpu.VMEM((n_y, tokens // 2, 128), BF16),
            dma((10,)),
            dma((4,)),
            dma((2, far + 1, len(ORDER))),
            dma((2, far + 1, len(ORDER))),
            dma((nz,)),
            dma((nz,)),
            dma((2, far + 1)),
            dma((2, far + 1)),
            dma((2,)),
            dma((2,)),
            dma((2,)),
            dma((n_y // 2, NX)),
            dma((n_y // 2, NX)),
            dma((n_y // 2, 2)),
            dma((n_y // 2, 2)),
        ],
        compiler_params=pltpu.CompilerParams(
            collective_id=0, has_side_effects=True, vmem_limit_bytes=56 * 1024 * 1024
        ),
    )(*args)
    outs = pl.pallas_call(
        deliver,
        name="deliver",
        out_shape=[jax.ShapeDtypeStruct(v.shape, v.dtype) for v in outs],
        in_specs=[vm] * 7,
        out_specs=[hbm] * 7,
        scratch_shapes=[dma((7,))],
        compiler_params=pltpu.CompilerParams(vmem_limit_bytes=1024 * 1024),
    )(*[pltpu.with_memory_space_constraint(v, pltpu.VMEM) for v in outs])
    full = [v.reshape(1, hidden, width) for v in outs[:3]]
    return (*full, *[v.T for v in outs[3:]])


def solution(mesh):
    placed = (
        P(None, "fs", "tp"),
        P(None, "fs", "tp"),
        P(None, "fs", "tp"),
        P("fs", "tp"),
        P("fs", "tp"),
        P("fs", "tp"),
        P("tp"),
        P("fs", None),
        P("fs", None),
        P("fs", None),
    )
    return jax.shard_map(
        on_device,
        mesh=mesh,
        in_specs=placed,
        out_specs=(
            P("tp", None, None),
            P("tp", None, None),
            P("tp", None, None),
            P(None, "tp"),
            P(None, "tp"),
            P(None, "tp"),
            P("fs", "tp"),
        ),
        check_vma=False,
    )
```

```python
import functools

import jax
import jax.numpy as jnp
from jax import lax
from jax.experimental import pallas as pl
from jax.experimental.pallas import tpu as pltpu
from jax.sharding import PartitionSpec as P

EPSILON = 1e-06
ROUTED_SCALE = 2.5
MESH = pl.DeviceIdType.MESH
NX = 4
ROW = 64
PIECE = 16
ORDER = (0, 2, 1, 3)
F32, BF16 = jnp.float32, jnp.bfloat16


def nt(a, b):
    return lax.dot_general(a, b, (((1,), (1,)), ((), ())), preferred_element_type=F32)


def tn(a, b):
    return lax.dot_general(a, b, (((0,), (0,)), ((), ())), preferred_element_type=F32)


def nn(a, b):
    return jnp.dot(a, b, preferred_element_type=F32)


def iota(shape, dim):
    return lax.broadcasted_iota(jnp.int32, shape, dim)


def silu(v):
    return v / (1.0 + jnp.exp(-v))


def halves(a, b):
    low = iota(a.shape, len(a.shape) - 1) < 64
    ax = len(a.shape) - 1
    return (
        jnp.where(low, a, pltpu.roll(b, 64, ax)),
        jnp.where(low, pltpu.roll(a, 64, ax), b),
    )


def kernel(
    n_tp, nz, units, cap,
    *refs,
):
    hbm_in, refs = refs[:10], refs[10:]
    outs, refs = refs[:7], refs[7:]
    inputs, refs = refs[:10], refs[10:]
    body(n_tp, nz, units, cap, hbm_in, *inputs, *outs, *refs)


def body(
    n_tp, nz, units, cap, hbm_in,
    tg, tu, td, sg, su, sd, gain, tok, ids, scores,
    o_gate, o_up, o_down, o_sgate, o_sup, o_sdown, o_mix,
    packed, pick, send_a, recv_a, blocks, small, normed, rows, total, spread, slot_weight,
    pre_send, pre_recv, acts, sdown, send_x, recv_x, send_y, recv_y,
    sem_in, sem_a, sem_ring_s, sem_ring_r, sem_pair_s, sem_pair_r,
    sem_small_s, sem_small_r, sem_spair, sem_j, sem_act, sem_x_s, sem_x_r, sem_y_s, sem_y_r,
):
    n_y = n_tp // NX
    far = nz // 2
    groups = nz // 4
    group_rows = 8 * units
    hidden = nz * 2 * units
    per_j = pre_send.shape[1]
    width = total.shape[1]
    tokens = tok.shape[0]
    me = lax.axis_index("tp")
    fs = lax.axis_index("fs")
    z, core = fs // 2, lax.rem(fs, 2)
    y, x = me // NX, lax.rem(me, NX)
    ahead = lax.rem(z + 1, nz) * 2 + core
    behind = lax.rem(z + nz - 1, nz) * 2 + core
    twin = z * 2 + 1 - core

    barrier = pltpu.get_barrier_semaphore()

    away = [(min(i, n_y - i) + min(j, NX - j), i, j) for i in range(n_y) for j in range(NX)]
    away = [
        lax.rem(y + i, n_y) * NX + lax.rem(x + j, NX)
        for distance, i, j in sorted(away, reverse=True)
        if distance
    ]
    vmem_in = (tg, tu, td, sg, su, sd, gain, tok, ids, scores)
    loads = [pltpu.make_async_copy(hbm_in[i], vmem_in[i], sem_in.at[i]) for i in range(10)]
    for load in loads:
        load.start()
    for other in (ahead, behind, twin):
        pl.semaphore_signal(barrier, inc=1, device_id={"fs": other}, device_id_type=MESH)
    for peer in away:
        pl.semaphore_signal(barrier, inc=1, device_id={"tp": peer}, device_id_type=MESH)
    for i in (0, 1, 2, 3, 4, 5, 6):
        loads[i].wait()

    scale = gain[...]

    with jax.named_scope("pack"):

        def unit(r):
            if r < units:
                return tg[r] * scale
            if r < 2 * units:
                return tu[r - units] * scale
            return td[r - 2 * units] if r < 3 * units else jnp.zeros((n_tp, 64), F32)

        parts = [sg[...] * scale, su[...] * scale, sd[...]]
        stack = jnp.concatenate([*parts, jnp.zeros((ROW - 3 * units, 64), F32)], axis=0)
        stack = jnp.concatenate([stack[: ROW // 2], stack[ROW // 2 :]], axis=1)
        small[z, core] = stack.astype(BF16)
        for r in range(0, ROW // 2, 8):
            several = [
                jnp.concatenate([unit(i), unit(i + ROW // 2)], axis=1) for i in range(r, r + 8)
            ]
            packed[:, pl.ds(r, 8), :] = jnp.swapaxes(jnp.stack(several, axis=0), 0, 1)
        for h in (0, 1):
            send_a[h] = packed[:, pl.ds(PIECE * h, PIECE), :].astype(BF16)
            recv_a[h, me] = send_a[h, me]
    with jax.named_scope("entry"):
        pl.semaphore_wait(barrier, n_tp + 2)

    def plane(src, dst, sems, peer, at=0):
        return pltpu.make_async_remote_copy(
            src_ref=src, dst_ref=dst, send_sem=sems.at[at], recv_sem=sems.at[at + 1],
            device_id={"tp": peer}, device_id_type=MESH,
        )

    def plane_done(ref, sems, at=0):
        piece = ref.at[pl.ds(0, n_tp - 1)]
        done = plane(piece, piece, sems, lax.rem(me + 1, n_tp), at)
        done.wait_send()
        done.wait_recv()

    def small_hop(d, s, at):
        return pltpu.make_async_remote_copy(
            src_ref=small.at[at, core], dst_ref=small.at[at, core],
            send_sem=sem_small_s.at[d], recv_sem=sem_small_r.at[d, s - 1],
            device_id={"fs": ahead if d == 0 else behind}, device_id_type=MESH,
        )

    def small_pair(at):
        return pltpu.make_async_remote_copy(
            src_ref=small.at[at, core], dst_ref=small.at[at, core],
            send_sem=sem_spair.at[0], recv_sem=sem_spair.at[1],
            device_id={"fs": twin}, device_id_type=MESH,
        )

    def origin(d, s):
        return lax.rem(z + nz - s, nz) if d == 0 else lax.rem(z + s, nz)

    small_hop(0, 1, z).start()
    small_hop(1, 1, z).start()
    small_pair(z).start()

    for h in (0, 1):
        for peer in away:
            plane(send_a.at[h, peer], recv_a.at[h, me], sem_a, peer, 2 * h).start()

    def small_step(s):
        for d in (0, 1):

            def arrived(d=d):
                at = origin(d, s)
                small_hop(d, s, at).wait_recv()
                small_pair(at).start()

                @pl.when((s + 1 < far) | ((s + 1 == far) & (d == 0)))
                def _():
                    small_hop(d, s + 1, at).start()

            if d == 0:
                arrived()
            else:
                pl.when(s < far)(arrived)

    for i in (7, 8, 9):
        loads[i].wait()
    tf = tok[...].astype(F32)
    normed[...] = (
        tf * lax.rsqrt(jnp.mean(tf * tf, axis=1, keepdims=True) + EPSILON)
    ).astype(BF16)
    ids_v, sc = ids[...], scores[...]
    ratio = ROUTED_SCALE * sc / jnp.sum(sc, axis=0, keepdims=True)
    expert_row = iota((128, tokens), 0)
    present = jnp.zeros((128, tokens), F32)
    weight_row = jnp.zeros((1, tokens), F32)
    for k in range(ids.shape[0]):
        present = jnp.where(ids_v[k : k + 1] == expert_row, 1.0, present)
        weight_row += jnp.where(ids_v[k : k + 1] == me, ratio[k : k + 1], 0.0)
    before = jnp.where(iota((tokens, tokens), 0) < iota((tokens, tokens), 1), 1.0, 0.0)
    position = nn(present.astype(BF16), before.astype(BF16))
    slots = jnp.where(present > 0.0, position, -1.0)
    slot_row = jnp.sum(jnp.where(expert_row == me, slots, 0.0), axis=0, keepdims=True)
    slot = slots.T
    lane = iota((tokens, 128), 1)
    taken = slot_row == iota((cap, tokens), 0).astype(F32)
    slot_weight[...] = jnp.broadcast_to(
        jnp.sum(jnp.where(taken, weight_row, 0.0), axis=1, keepdims=True), slot_weight.shape
    )
    rows[...] = nn(jnp.where(taken, 1.0, 0.0).astype(BF16), normed[...]).astype(BF16)
    for i in range(NX):
        col = jnp.sum(jnp.where(lane == y * NX + i, slot, 0.0), axis=1, keepdims=True)
        spread[i] = jnp.where(col == iota((tokens, cap), 1).astype(F32), 1.0, 0.0).astype(BF16)
    total[...] = jnp.zeros_like(total)

    shape = (group_rows, 8 * ROW)
    i, f, r = iota(shape, 0), iota(shape, 1) // ROW, iota(shape, 1) & (ROW - 1)
    ordered = []
    for m in range(3):
        inside = (r >= units * m) & (r < units * (m + 1))
        ordered.append(jnp.where(inside & (i == units * f + r - units * m), 1.0, 0.0))
    pick[...] = jnp.concatenate(ordered, axis=0).astype(BF16)

    def hop(d, s, q, at):
        piece = blocks.at[at, core, pl.ds(q * PIECE, PIECE)]
        return pltpu.make_async_remote_copy(
            src_ref=piece, dst_ref=piece,
            send_sem=sem_ring_s.at[d, q], recv_sem=sem_ring_r.at[d, s - 1, q],
            device_id={"fs": ahead if d == 0 else behind}, device_id_type=MESH,
        )

    def pair(at, q=None):
        block = blocks.at[at, core]
        piece = block if q is None else blocks.at[at, core, pl.ds(q * PIECE, PIECE)]
        return pltpu.make_async_remote_copy(
            src_ref=piece, dst_ref=piece,
            send_sem=sem_pair_s, recv_sem=sem_pair_r.at[lax.rem(at + nz - z, nz)],
            device_id={"fs": twin}, device_id_type=MESH,
        )

    early = 3
    with jax.named_scope("small_early"):
        for i in range(1, early + 1):
            small_step(i)
    for h in (0, 1):
        with jax.named_scope(f"await_weights{h}"):
            plane_done(recv_a.at[h], sem_a, 2 * h)
        with jax.named_scope("unpack"):
            for m in range(n_tp // 2):
                upper, lower = recv_a[h, 2 * m].astype(F32), recv_a[h, 2 * m + 1].astype(F32)
                for part, v in enumerate(halves(upper, lower)):
                    at = pl.ds(PIECE * (h + 2 * part), PIECE)
                    blocks[z, core, at, pl.ds(128 * m, 128)] = v.astype(BF16)
        for q in ORDER[2 * h : 2 * h + 2]:
            for d in (0, 1):
                hop(d, 1, q, z).start()
            pair(z, q).start()

    def last_leg(d, q):
        return (q in ORDER[:2]) == (d == 0)

    def activated(*ats):
        with jax.named_scope("await_pair"):
            for at in ats:
                pair(at).wait_recv()
        w = jnp.concatenate([blocks[at].reshape(2 * ROW, width) for at in ats], axis=0)
        pre = nt(rows[...], w)
        act = silu(pltpu.roll(pre, 2 * units, 1)) * pltpu.roll(pre, units, 1)
        unit = iota(act.shape, 1) & (ROW - 1)
        return jnp.where((unit >= 2 * units) & (unit < 3 * units), act, 0.0).astype(BF16)

    def expert(*ats):
        act = activated(*ats)
        w = jnp.concatenate([blocks[at].reshape(2 * ROW, width) for at in ats], axis=0)
        total[...] += nn(act, w)

    def padded(v):
        spare = jnp.zeros((-hidden % 128, 128), F32)
        return jnp.concatenate([v, spare], axis=0)

    def shared_rows():
        got = [[], [], []]
        for g in range(groups):
            v = small[pl.ds(4 * g, 4)].reshape(8, ROW // 2, 128).astype(F32)
            v = jnp.concatenate([v, pltpu.roll(v, 64, 2)], axis=1).reshape(8 * ROW, 128)
            v = v.astype(BF16)
            found = nn(pick[...], v)
            for m in range(3):
                got[m].append(found[group_rows * m : group_rows * (m + 1)])
        gate, up, down = [jnp.concatenate(one, axis=0) for one in got]
        for o, v in ((o_sgate, gate), (o_sup, up), (o_sdown, down)):
            o[...] = padded(v).T[:64, :hidden].astype(BF16)
        pad = jnp.zeros((n_tp * per_j - hidden, 128), F32)
        both = jnp.concatenate([halves(gate, up)[0], pad], axis=0)
        pre_send[...] = both.astype(BF16).reshape(n_tp, per_j, 128)
        low = iota(down.shape, 1) < 64
        down = jnp.concatenate([jnp.where(low, down, 0.0), pad], axis=0)
        sdown[...] = down.astype(BF16)
        pre_recv[me] = pre_send[me]

        def send(i, _):
            peer = lax.rem(me + i, n_tp)
            plane(pre_send.at[peer], pre_recv.at[me], sem_j, peer).start()
            return 0

        lax.fori_loop(1, n_tp, send, 0)

    def shared_acts():
        with jax.named_scope("await_j"):
            plane_done(pre_recv, sem_j)
        gates, ups = [], []
        for m in range(n_tp // 2):
            g, u = halves(pre_recv[2 * m].astype(F32), pre_recv[2 * m + 1].astype(F32))
            gates.append(g.astype(BF16))
            ups.append(u.astype(BF16))
        gate = nt(jnp.concatenate(gates, axis=1), normed[...])
        up = nt(jnp.concatenate(ups, axis=1), normed[...])
        acts[me] = (silu(gate) * up).astype(BF16)

        def send_act(i, _):
            peer = lax.rem(me + i, n_tp)
            plane(acts.at[me], acts.at[me], sem_act, peer).start()
            return 0

        lax.fori_loop(1, n_tp, send_act, 0)

    def ring_step(s, _):
        for n, q in enumerate(ORDER):
            for d in (0, 1):
                at = origin(d, s)
                with jax.named_scope(f"arrive{d}{n}"):
                    hop(d, s, q, at).wait_recv()
                if last_leg(d, q):
                    hop(d, s + 1, q, at).start()
                else:

                    @pl.when(s + 1 < far)
                    def _(d=d, q=q, at=at):
                        hop(d, s + 1, q, at).start()

                pair(at, q).start()

            if n == 1:

                @pl.when(s + early <= far)
                def _():
                    with jax.named_scope("small"):
                        small_step(s + early)

                @pl.when(s == far - early + 1)
                def _():
                    with jax.named_scope("await_small"):
                        everything = small.at[:, 0]
                        done = pltpu.make_async_remote_copy(
                            src_ref=everything, dst_ref=everything,
                            send_sem=sem_spair.at[0], recv_sem=sem_spair.at[1],
                            device_id={"fs": twin}, device_id_type=MESH,
                        )
                        done.wait_send()
                        done.wait_recv()
                    with jax.named_scope("shared_rows"):
                        shared_rows()

            if n == 2:

                @pl.when(s == far - 1)
                def _():
                    with jax.named_scope("expert_in"):
                        expert(origin(0, s - 1), origin(1, s - 1))

        @pl.when(s == 1)
        def _():
            with jax.named_scope("expert_own"):
                expert(z)

        @pl.when((s > 1) & (s < far - 1))
        def _():
            with jax.named_scope("expert"):
                expert(origin(0, s - 1), origin(1, s - 1))

        return 0

    lax.fori_loop(1, far, ring_step, 0)
    opposite = lax.rem(z + far, nz)
    with jax.named_scope("shared_acts"):
        shared_acts()
    with jax.named_scope("expert_near"):
        expert(origin(0, far - 1), origin(1, far - 1))
    with jax.named_scope("arrive_last"):
        for q in ORDER:
            hop(0 if q in ORDER[:2] else 1, far, q, opposite).wait_recv()
            pair(opposite, q).start()
    with jax.named_scope("expert_last"):
        act = activated(opposite)

    def sent(ref, sem):
        pltpu.make_async_remote_copy(
            src_ref=ref, dst_ref=ref, send_sem=sem, recv_sem=sem_pair_r.at[0],
            device_id={"fs": twin}, device_id_type=MESH,
        ).wait_send()

    def drain():
        for d in (0, 1):
            for q in ORDER:
                hops = far - 1 + last_leg(d, q)
                sent(blocks.at[pl.ds(0, hops), 0, pl.ds(0, PIECE)], sem_ring_s.at[d, q])
            sent(small.at[pl.ds(0, far - d), 0], sem_small_s.at[d])
        sent(blocks.at[:, 0], sem_pair_s)
        sent(send_x.at[pl.ds(0, NX - 1)], sem_x_s)

    w = slot_weight[...]
    pairs = n_y // 2
    turns = [(pairs // 2 + (i + 1) // 2 * (1 if i % 2 else -1)) % pairs for i in range(pairs)]
    turns = [i for i in turns if i] + [0]

    def quarter(k):
        return lax.rem(y // 2 + turns[k], pairs)

    def row_copy(k, i):
        to = lax.rem(x + i, NX)
        return pltpu.make_async_remote_copy(
            src_ref=send_x.at[to, k], dst_ref=recv_x.at[x, k],
            send_sem=sem_x_s, recv_sem=sem_x_r.at[k, i],
            device_id={"tp": y * NX + to}, device_id_type=MESH,
        )

    for k in range(pairs):
        p = quarter(k)
        for h in range(NX // 2):
            several = []
            for i in (2 * p, 2 * p + 1):
                cols = pl.ds(pl.multiple_of(128 * (i * (NX // 2) + h), 128), 128)
                new = nn(act, blocks[opposite, :, :, cols].reshape(2 * ROW, 128))
                several.append((total[:, cols] + new) * w)
            for i, v in enumerate(halves(*several)):
                send_x[2 * h + i, k] = v.astype(BF16)
        for i in (2, 1, 3) if NX == 4 else range(1, NX):
            row_copy(k, i).start()
        recv_x[x, k] = send_x[x, k]

    part = min(512, width)
    results = (o_gate, o_up, o_down)

    def served(g):
        def some(n, _):
            cols = pl.ds(pl.multiple_of(n * part, part), part)
            v = blocks[pl.ds(4 * g, 4), :, :, cols].reshape(8 * ROW, part)
            v = nn(pick[...], v)
            for m in range(3):
                results[m][g, :, cols] = v[group_rows * m : group_rows * (m + 1)].astype(BF16)
            return 0

        with jax.named_scope("served"):
            lax.fori_loop(0, width // part, some, 0)

    for g in range(groups - 1):
        served(g)

    half = tokens // 2
    odd = lax.rem(y, 2)

    def col_copy(k, h):
        last = k == pairs - 1
        to = 2 * quarter(k) + (1 - odd if last else h)
        return pltpu.make_async_remote_copy(
            src_ref=send_y.at[to], dst_ref=recv_y.at[y],
            send_sem=sem_y_s, recv_sem=sem_y_r.at[k, 0 if last else odd],
            device_id={"tp": to * NX + x}, device_id_type=MESH,
        )

    def col_arrival(k, h):
        return pltpu.make_async_remote_copy(
            src_ref=recv_y.at[0], dst_ref=recv_y.at[0],
            send_sem=sem_y_s, recv_sem=sem_y_r.at[k, h],
            device_id={"tp": lax.rem(me + 1, n_tp)}, device_id_type=MESH,
        )

    y_copies = [(k, h) for k in range(pairs) for h in (0, 1) if k < pairs - 1 or h == 0]
    for k in range(pairs):
        with jax.named_scope(f"await_x{k}"):
            for i in range(1, NX):
                row_copy(k, i).wait_recv()
        acc = jnp.zeros((tokens, 128), F32)
        for i in range(NX):
            acc += nn(spread[i], recv_x[i, k])
        for h, v in enumerate(halves(acc[:half], acc[half:])):
            send_y[2 * quarter(k) + h] = v.astype(BF16)
        for h in (0, 1):
            if (k, h) in y_copies:
                col_copy(k, h).start()
    recv_y[y] = send_y[y]
    served(groups - 1)
    with jax.named_scope("drain"):
        drain()

    with jax.named_scope("await_act"):
        plane_done(acts, sem_act)
    shared = tn(acts[...].reshape(n_tp * per_j, tokens), sdown[...])
    mixed = halves(shared[:half], shared[half:])[0]
    with jax.named_scope("await_y"):
        for k, h in y_copies:
            col_arrival(k, h).wait_recv()
    for i in range(n_y):
        mixed += recv_y[i].astype(F32)
    mixed = mixed.T
    o_mix[...] = jnp.concatenate([mixed[:64], mixed[64:]], axis=1).astype(BF16)

    sent(send_y.at[pl.ds(0, n_y - 1)], sem_y_s)


def deliver(*refs):
    n = (len(refs) - 1) // 2
    copies = [pltpu.make_async_copy(refs[i], refs[n + i], refs[-1].at[i]) for i in range(n)]
    for copy in copies:
        copy.start()
    for copy in copies:
        copy.wait()


def on_device(*args):
    n_tp, units = args[0].shape[:2]
    nz = lax.axis_size("fs") // 2
    tokens, width = args[7].shape
    top = args[8].shape[1]
    cap = min(tokens, 5 * tokens * top // (2 * n_tp))
    hidden = nz * 2 * units
    per_j = -(-hidden // (16 * n_tp)) * 16
    n_y = n_tp // NX
    far = nz // 2
    groups = nz // 4
    args = [jnp.swapaxes(v, 0, 1) for v in args[:3]] + list(args[3:])
    args[6] = args[6].reshape(1, -1)
    args[8:] = [v.T for v in args[8:]]
    vm = pl.BlockSpec(memory_space=pltpu.VMEM)
    hbm = pl.BlockSpec(memory_space=pl.ANY)
    dma = pltpu.SemaphoreType.DMA
    big = pltpu.VMEM((groups, 8 * units, width), BF16)
    thin = pltpu.VMEM((64, hidden), BF16)
    mix = pltpu.VMEM((64, tokens), BF16)
    outs = pl.pallas_call(
        functools.partial(kernel, n_tp, nz, units, cap),
        name="hand_over",
        out_shape=[big, big, big, thin, thin, thin, mix],
        in_specs=[hbm] * 10,
        out_specs=[vm] * 7,
        scratch_shapes=[
            *[pltpu.VMEM(v.shape, v.dtype) for v in args],
            pltpu.VMEM((n_tp, ROW // 2, 128), F32),
            pltpu.VMEM((24 * units, 8 * ROW), BF16),
            pltpu.VMEM((2, n_tp, PIECE, 128), BF16),
            pltpu.VMEM((2, n_tp, PIECE, 128), BF16),
            pltpu.VMEM((nz, 2, ROW, width), BF16),
            pltpu.VMEM((nz, 2, ROW // 2, 128), BF16),
            pltpu.VMEM((tokens, width), BF16),
            pltpu.VMEM((cap, width), BF16),
            pltpu.VMEM((cap, width), F32),
            pltpu.VMEM((NX, tokens, cap), BF16),
            pltpu.VMEM((cap, 128), F32),
            pltpu.VMEM((n_tp, per_j, 128), BF16),
            pltpu.VMEM((n_tp, per_j, 128), BF16),
            pltpu.VMEM((n_tp, per_j, tokens), BF16),
            pltpu.VMEM((n_tp * per_j, 128), BF16),
            pltpu.VMEM((NX, n_y // 2, cap, 128), BF16),
            pltpu.VMEM((NX, n_y // 2, cap, 128), BF16),
            pltpu.VMEM((n_y, tokens // 2, 128), BF16),
            pltpu.VMEM((n_y, tokens // 2, 128), BF16),
            dma((10,)),
            dma((4,)),
            dma((2, len(ORDER))),
            dma((2, far, len(ORDER))),
            dma(()),
            dma((nz,)),
            dma((2,)),
            dma((2, far)),
            dma((2,)),
            dma((2,)),
            dma((2,)),
            dma(()),
            dma((n_y // 2, NX)),
            dma(()),
            dma((n_y // 2, 2)),
        ],
        compiler_params=pltpu.CompilerParams(
            collective_id=0, has_side_effects=True, vmem_limit_bytes=56 * 1024 * 1024
        ),
    )(*args)
    outs = pl.pallas_call(
        deliver,
        name="deliver",
        out_shape=[jax.ShapeDtypeStruct(v.shape, v.dtype) for v in outs],
        in_specs=[vm] * 7,
        out_specs=[hbm] * 7,
        scratch_shapes=[dma((7,))],
        compiler_params=pltpu.CompilerParams(vmem_limit_bytes=1024 * 1024),
    )(*[pltpu.with_memory_space_constraint(v, pltpu.VMEM) for v in outs])
    full = [v.reshape(1, hidden, width) for v in outs[:3]]
    return (*full, *[v.T for v in outs[3:]])


def solution(mesh):
    placed = (
        P(None, "fs", "tp"),
        P(None, "fs", "tp"),
        P(None, "fs", "tp"),
        P("fs", "tp"),
        P("fs", "tp"),
        P("fs", "tp"),
        P("tp"),
        P("fs", None),
        P("fs", None),
        P("fs", None),
    )
    return jax.shard_map(
        on_device,
        mesh=mesh,
        in_specs=placed,
        out_specs=(
            P("tp", None, None),
            P("tp", None, None),
            P("tp", None, None),
            P(None, "tp"),
            P(None, "tp"),
            P(None, "tp"),
            P("fs", "tp"),
        ),
        check_vma=False,
    )
```

```python
import functools

import jax
import jax.numpy as jnp
from jax import lax
from jax.experimental import pallas as pl
from jax.experimental.pallas import tpu as pltpu
from jax.sharding import PartitionSpec as P

EPSILON = 1e-06
ROUTED_SCALE = 2.5
MESH = pl.DeviceIdType.MESH
NX = 4
ROW = 64
PIECE = 16
ORDER = (0, 2, 1, 3)
F32, BF16 = jnp.float32, jnp.bfloat16


def nt(a, b):
    return lax.dot_general(a, b, (((1,), (1,)), ((), ())), preferred_element_type=F32)


def tn(a, b):
    return lax.dot_general(a, b, (((0,), (0,)), ((), ())), preferred_element_type=F32)


def nn(a, b):
    return jnp.dot(a, b, preferred_element_type=F32)


def iota(shape, dim):
    return lax.broadcasted_iota(jnp.int32, shape, dim)


def silu(v):
    return v / (1.0 + jnp.exp(-v))


def halves(a, b):
    low = iota(a.shape, len(a.shape) - 1) < 64
    ax = len(a.shape) - 1
    return (
        jnp.where(low, a, pltpu.roll(b, 64, ax)),
        jnp.where(low, pltpu.roll(a, 64, ax), b),
    )


def kernel(
    n_tp, nz, units, cap,
    *refs,
):
    hbm_in, refs = refs[:10], refs[10:]
    outs, refs = refs[:7], refs[7:]
    inputs, refs = refs[:10], refs[10:]
    body(n_tp, nz, units, cap, hbm_in, *inputs, *outs, *refs)


def body(
    n_tp, nz, units, cap, hbm_in,
    tg, tu, td, sg, su, sd, gain, tok, ids, scores,
    o_gate, o_up, o_down, o_sgate, o_sup, o_sdown, o_mix,
    packed, pick, send_a, recv_a, blocks, small, normed, rows, total, spread, slot_weight,
    pre_send, pre_recv, acts, sdown, send_x, recv_x, send_y, recv_y,
    sem_in, sem_a, sem_ring_s, sem_ring_r, sem_pair_s, sem_pair_r,
    sem_small_s, sem_small_r, sem_spair, sem_j, sem_act, sem_x_s, sem_x_r, sem_y_s, sem_y_r,
):
    n_y = n_tp // NX
    far = nz // 2
    groups = nz // 4
    group_rows = 8 * units
    hidden = nz * 2 * units
    per_j = pre_send.shape[1]
    width = total.shape[1]
    tokens = tok.shape[0]
    me = lax.axis_index("tp")
    fs = lax.axis_index("fs")
    z, core = fs // 2, lax.rem(fs, 2)
    y, x = me // NX, lax.rem(me, NX)
    ahead = lax.rem(z + 1, nz) * 2 + core
    behind = lax.rem(z + nz - 1, nz) * 2 + core
    twin = z * 2 + 1 - core

    barrier = pltpu.get_barrier_semaphore()

    away = [(min(i, n_y - i) + min(j, NX - j), i, j) for i in range(n_y) for j in range(NX)]
    away = [
        lax.rem(y + i, n_y) * NX + lax.rem(x + j, NX)
        for distance, i, j in sorted(away, reverse=True)
        if distance
    ]
    vmem_in = (tg, tu, td, sg, su, sd, gain, tok, ids, scores)
    loads = [pltpu.make_async_copy(hbm_in[i], vmem_in[i], sem_in.at[i]) for i in range(10)]
    for load in loads:
        load.start()
    for other in (ahead, behind, twin):
        pl.semaphore_signal(barrier, inc=1, device_id={"fs": other}, device_id_type=MESH)
    for peer in away:
        pl.semaphore_signal(barrier, inc=1, device_id={"tp": peer}, device_id_type=MESH)
    for i in (0, 1, 2, 3, 4, 5, 6):
        loads[i].wait()

    scale = gain[...]

    with jax.named_scope("pack"):

        def unit(r):
            if r < units:
                return tg[r] * scale
            if r < 2 * units:
                return tu[r - units] * scale
            return td[r - 2 * units] if r < 3 * units else jnp.zeros((n_tp, 64), F32)

        parts = [sg[...] * scale, su[...] * scale, sd[...]]
        stack = jnp.concatenate([*parts, jnp.zeros((ROW - 3 * units, 64), F32)], axis=0)
        stack = jnp.concatenate([stack[: ROW // 2], stack[ROW // 2 :]], axis=1)
        small[z, core] = stack.astype(BF16)
        for r in range(0, ROW // 2, 8):
            several = [
                jnp.concatenate([unit(i), unit(i + ROW // 2)], axis=1) for i in range(r, r + 8)
            ]
            packed[:, pl.ds(r, 8), :] = jnp.swapaxes(jnp.stack(several, axis=0), 0, 1)
        for h in (0, 1):
            send_a[h] = packed[:, pl.ds(PIECE * h, PIECE), :].astype(BF16)
            recv_a[h, me] = send_a[h, me]
    with jax.named_scope("entry"):
        pl.semaphore_wait(barrier, n_tp + 2)

    def plane(src, dst, sems, peer, at=0):
        return pltpu.make_async_remote_copy(
            src_ref=src, dst_ref=dst, send_sem=sems.at[at], recv_sem=sems.at[at + 1],
            device_id={"tp": peer}, device_id_type=MESH,
        )

    def plane_done(ref, sems, at=0):
        piece = ref.at[pl.ds(0, n_tp - 1)]
        done = plane(piece, piece, sems, lax.rem(me + 1, n_tp), at)
        done.wait_send()
        done.wait_recv()

    def small_hop(d, s, at):
        return pltpu.make_async_remote_copy(
            src_ref=small.at[at, core], dst_ref=small.at[at, core],
            send_sem=sem_small_s.at[d], recv_sem=sem_small_r.at[d, s - 1],
            device_id={"fs": ahead if d == 0 else behind}, device_id_type=MESH,
        )

    def small_pair(at):
        return pltpu.make_async_remote_copy(
            src_ref=small.at[at, core], dst_ref=small.at[at, core],
            send_sem=sem_spair.at[0], recv_sem=sem_spair.at[1],
            device_id={"fs": twin}, device_id_type=MESH,
        )

    def origin(d, s):
        return lax.rem(z + nz - s, nz) if d == 0 else lax.rem(z + s, nz)

    small_hop(0, 1, z).start()
    small_hop(1, 1, z).start()
    small_pair(z).start()

    for h in (0, 1):
        for peer in away:
            plane(send_a.at[h, peer], recv_a.at[h, me], sem_a, peer, 2 * h).start()

    def small_step(s):
        for d in (0, 1):

            def arrived(d=d):
                at = origin(d, s)
                small_hop(d, s, at).wait_recv()
                small_pair(at).start()

                @pl.when((s + 1 < far) | ((s + 1 == far) & (d == 0)))
                def _():
                    small_hop(d, s + 1, at).start()

            if d == 0:
                arrived()
            else:
                pl.when(s < far)(arrived)

    for i in (7, 8, 9):
        loads[i].wait()
    tf = tok[...].astype(F32)
    normed[...] = (
        tf * lax.rsqrt(jnp.mean(tf * tf, axis=1, keepdims=True) + EPSILON)
    ).astype(BF16)
    ids_v, sc = ids[...], scores[...]
    ratio = ROUTED_SCALE * sc / jnp.sum(sc, axis=0, keepdims=True)
    expert_row = iota((128, tokens), 0)
    present = jnp.zeros((128, tokens), F32)
    weight_row = jnp.zeros((1, tokens), F32)
    for k in range(ids.shape[0]):
        present = jnp.where(ids_v[k : k + 1] == expert_row, 1.0, present)
        weight_row += jnp.where(ids_v[k : k + 1] == me, ratio[k : k + 1], 0.0)
    before = jnp.where(iota((tokens, tokens), 0) < iota((tokens, tokens), 1), 1.0, 0.0)
    position = nn(present.astype(BF16), before.astype(BF16))
    slots = jnp.where(present > 0.0, position, -1.0)
    slot_row = jnp.sum(jnp.where(expert_row == me, slots, 0.0), axis=0, keepdims=True)
    slot = slots.T
    lane = iota((tokens, 128), 1)
    taken = slot_row == iota((cap, tokens), 0).astype(F32)
    slot_weight[...] = jnp.broadcast_to(
        jnp.sum(jnp.where(taken, weight_row, 0.0), axis=1, keepdims=True), slot_weight.shape
    )
    rows[...] = nn(jnp.where(taken, 1.0, 0.0).astype(BF16), normed[...]).astype(BF16)
    for i in range(NX):
        col = jnp.sum(jnp.where(lane == y * NX + i, slot, 0.0), axis=1, keepdims=True)
        spread[i] = jnp.where(col == iota((tokens, cap), 1).astype(F32), 1.0, 0.0).astype(BF16)
    total[...] = jnp.zeros_like(total)

    shape = (group_rows, 8 * ROW)
    i, f, r = iota(shape, 0), iota(shape, 1) // ROW, iota(shape, 1) & (ROW - 1)
    ordered = []
    for m in range(3):
        inside = (r >= units * m) & (r < units * (m + 1))
        ordered.append(jnp.where(inside & (i == units * f + r - units * m), 1.0, 0.0))
    pick[...] = jnp.concatenate(ordered, axis=0).astype(BF16)

    def hop(d, s, q, at):
        piece = blocks.at[at, core, pl.ds(q * PIECE, PIECE)]
        return pltpu.make_async_remote_copy(
            src_ref=piece, dst_ref=piece,
            send_sem=sem_ring_s.at[d, q], recv_sem=sem_ring_r.at[d, s - 1, q],
            device_id={"fs": ahead if d == 0 else behind}, device_id_type=MESH,
        )

    def pair(at, q=None):
        block = blocks.at[at, core]
        piece = block if q is None else blocks.at[at, core, pl.ds(q * PIECE, PIECE)]
        return pltpu.make_async_remote_copy(
            src_ref=piece, dst_ref=piece,
            send_sem=sem_pair_s, recv_sem=sem_pair_r.at[lax.rem(at + nz - z, nz)],
            device_id={"fs": twin}, device_id_type=MESH,
        )

    early = 3
    with jax.named_scope("small_early"):
        for i in range(1, early):
            small_step(i)
    for h in (0, 1):
        if h:
            with jax.named_scope("small_between"):
                small_step(early)
        with jax.named_scope(f"await_weights{h}"):
            plane_done(recv_a.at[h], sem_a, 2 * h)
        with jax.named_scope("unpack"):
            for m in range(n_tp // 2):
                upper, lower = recv_a[h, 2 * m].astype(F32), recv_a[h, 2 * m + 1].astype(F32)
                for part, v in enumerate(halves(upper, lower)):
                    at = pl.ds(PIECE * (h + 2 * part), PIECE)
                    blocks[z, core, at, pl.ds(128 * m, 128)] = v.astype(BF16)
        for q in ORDER[2 * h : 2 * h + 2]:
            for d in (0, 1):
                hop(d, 1, q, z).start()
            pair(z, q).start()

    def last_leg(d, q):
        return (q in ORDER[:2]) == (d == 0)

    def activated(*ats):
        with jax.named_scope("await_pair"):
            for at in ats:
                pair(at).wait_recv()
        w = jnp.concatenate([blocks[at].reshape(2 * ROW, width) for at in ats], axis=0)
        pre = nt(rows[...], w)
        act = silu(pltpu.roll(pre, 2 * units, 1)) * pltpu.roll(pre, units, 1)
        unit = iota(act.shape, 1) & (ROW - 1)
        return jnp.where((unit >= 2 * units) & (unit < 3 * units), act, 0.0).astype(BF16)

    def expert(*ats):
        act = activated(*ats)
        w = jnp.concatenate([blocks[at].reshape(2 * ROW, width) for at in ats], axis=0)
        total[...] += nn(act, w)

    def padded(v):
        spare = jnp.zeros((-hidden % 128, 128), F32)
        return jnp.concatenate([v, spare], axis=0)

    def shared_rows():
        got = [[], [], []]
        for g in range(groups):
            v = small[pl.ds(4 * g, 4)].reshape(8, ROW // 2, 128).astype(F32)
            v = jnp.concatenate([v, pltpu.roll(v, 64, 2)], axis=1).reshape(8 * ROW, 128)
            v = v.astype(BF16)
            found = nn(pick[...], v)
            for m in range(3):
                got[m].append(found[group_rows * m : group_rows * (m + 1)])
        gate, up, down = [jnp.concatenate(one, axis=0) for one in got]
        for o, v in ((o_sgate, gate), (o_sup, up), (o_sdown, down)):
            o[...] = padded(v).T[:64, :hidden].astype(BF16)
        pad = jnp.zeros((n_tp * per_j - hidden, 128), F32)
        both = jnp.concatenate([halves(gate, up)[0], pad], axis=0)
        pre_send[...] = both.astype(BF16).reshape(n_tp, per_j, 128)
        low = iota(down.shape, 1) < 64
        down = jnp.concatenate([jnp.where(low, down, 0.0), pad], axis=0)
        sdown[...] = down.astype(BF16)
        pre_recv[me] = pre_send[me]

        def send(i, _):
            peer = lax.rem(me + i, n_tp)
            plane(pre_send.at[peer], pre_recv.at[me], sem_j, peer).start()
            return 0

        lax.fori_loop(1, n_tp, send, 0)

    def shared_acts():
        with jax.named_scope("await_j"):
            plane_done(pre_recv, sem_j)
        gates, ups = [], []
        for m in range(n_tp // 2):
            g, u = halves(pre_recv[2 * m].astype(F32), pre_recv[2 * m + 1].astype(F32))
            gates.append(g.astype(BF16))
            ups.append(u.astype(BF16))
        gate = nt(jnp.concatenate(gates, axis=1), normed[...])
        up = nt(jnp.concatenate(ups, axis=1), normed[...])
        acts[me] = (silu(gate) * up).astype(BF16)

        def send_act(i, _):
            peer = lax.rem(me + i, n_tp)
            plane(acts.at[me], acts.at[me], sem_act, peer).start()
            return 0

        lax.fori_loop(1, n_tp, send_act, 0)

    def ring_step(s, _):
        for n, q in enumerate(ORDER):
            for d in (0, 1):
                at = origin(d, s)
                with jax.named_scope(f"arrive{d}{n}"):
                    hop(d, s, q, at).wait_recv()
                if last_leg(d, q):
                    hop(d, s + 1, q, at).start()
                else:

                    @pl.when(s + 1 < far)
                    def _(d=d, q=q, at=at):
                        hop(d, s + 1, q, at).start()

                pair(at, q).start()

            if n == 1:

                @pl.when(s + early <= far)
                def _():
                    with jax.named_scope("small"):
                        small_step(s + early)

            if n == 3:

                @pl.when(s == far - early)
                def _():
                    with jax.named_scope("await_small"):
                        everything = small.at[:, 0]
                        done = pltpu.make_async_remote_copy(
                            src_ref=everything, dst_ref=everything,
                            send_sem=sem_spair.at[0], recv_sem=sem_spair.at[1],
                            device_id={"fs": twin}, device_id_type=MESH,
                        )
                        done.wait_send()
                        done.wait_recv()
                    with jax.named_scope("shared_rows"):
                        shared_rows()

            if n == 2:

                @pl.when(s == far - 1)
                def _():
                    with jax.named_scope("expert_in"):
                        expert(origin(0, s - 1), origin(1, s - 1))

        @pl.when(s == 1)
        def _():
            with jax.named_scope("expert_own"):
                expert(z)

        @pl.when((s > 1) & (s < far - 1))
        def _():
            with jax.named_scope("expert"):
                expert(origin(0, s - 1), origin(1, s - 1))

        return 0

    lax.fori_loop(1, far, ring_step, 0)
    opposite = lax.rem(z + far, nz)
    with jax.named_scope("shared_acts"):
        shared_acts()

    def take_last():
        for q in ORDER:
            hop(0 if q in ORDER[:2] else 1, far, q, opposite).wait_recv()
            pair(opposite, q).start()

    pl.when(core == 1)(take_last)
    with jax.named_scope("expert_near"):
        expert(origin(0, far - 1), origin(1, far - 1))
    pl.when(core == 0)(take_last)
    with jax.named_scope("expert_last"):
        act = activated(opposite)

    def sent(ref, sem):
        pltpu.make_async_remote_copy(
            src_ref=ref, dst_ref=ref, send_sem=sem, recv_sem=sem_pair_r.at[0],
            device_id={"fs": twin}, device_id_type=MESH,
        ).wait_send()

    def drain():
        for d in (0, 1):
            for q in ORDER:
                hops = far - 1 + last_leg(d, q)
                sent(blocks.at[pl.ds(0, hops), 0, pl.ds(0, PIECE)], sem_ring_s.at[d, q])
            sent(small.at[pl.ds(0, far - d), 0], sem_small_s.at[d])
        sent(blocks.at[:, 0], sem_pair_s)
        sent(send_x.at[pl.ds(0, NX - 1)], sem_x_s)

    w = slot_weight[...]
    pairs = n_y // 2
    turns = [(pairs // 2 + (i + 1) // 2 * (1 if i % 2 else -1)) % pairs for i in range(pairs)]
    turns = [i for i in turns if i] + [0]

    def quarter(k):
        return lax.rem(y // 2 + turns[k], pairs)

    def row_copy(k, i):
        to = lax.rem(x + i, NX)
        return pltpu.make_async_remote_copy(
            src_ref=send_x.at[to, k], dst_ref=recv_x.at[x, k],
            send_sem=sem_x_s, recv_sem=sem_x_r.at[k, i],
            device_id={"tp": y * NX + to}, device_id_type=MESH,
        )

    for k in range(pairs):
        p = quarter(k)
        for h in range(NX // 2):
            several = []
            for i in (2 * p, 2 * p + 1):
                cols = pl.ds(pl.multiple_of(128 * (i * (NX // 2) + h), 128), 128)
                new = nn(act, blocks[opposite, :, :, cols].reshape(2 * ROW, 128))
                several.append((total[:, cols] + new) * w)
            for i, v in enumerate(halves(*several)):
                send_x[2 * h + i, k] = v.astype(BF16)
        for i in (2, 1, 3) if NX == 4 else range(1, NX):
            row_copy(k, i).start()
        recv_x[x, k] = send_x[x, k]

    part = min(512, width)
    results = (o_gate, o_up, o_down)

    def served(g):
        def some(n, _):
            cols = pl.ds(pl.multiple_of(n * part, part), part)
            v = blocks[pl.ds(4 * g, 4), :, :, cols].reshape(8 * ROW, part)
            v = nn(pick[...], v)
            for m in range(3):
                results[m][g, :, cols] = v[group_rows * m : group_rows * (m + 1)].astype(BF16)
            return 0

        with jax.named_scope("served"):
            lax.fori_loop(0, width // part, some, 0)

    for g in range(groups - 1):
        served(g)

    half = tokens // 2
    odd = lax.rem(y, 2)

    def col_copy(k, h):
        last = k == pairs - 1
        to = 2 * quarter(k) + (1 - odd if last else h)
        return pltpu.make_async_remote_copy(
            src_ref=send_y.at[to], dst_ref=recv_y.at[y],
            send_sem=sem_y_s, recv_sem=sem_y_r.at[k, 0 if last else odd],
            device_id={"tp": to * NX + x}, device_id_type=MESH,
        )

    def col_arrival(k, h):
        return pltpu.make_async_remote_copy(
            src_ref=recv_y.at[0], dst_ref=recv_y.at[0],
            send_sem=sem_y_s, recv_sem=sem_y_r.at[k, h],
            device_id={"tp": lax.rem(me + 1, n_tp)}, device_id_type=MESH,
        )

    y_copies = [(k, h) for k in range(pairs) for h in (0, 1) if k < pairs - 1 or h == 0]
    for k in range(pairs):
        with jax.named_scope(f"await_x{k}"):
            for i in range(1, NX):
                row_copy(k, i).wait_recv()
        acc = jnp.zeros((tokens, 128), F32)
        for i in range(NX):
            acc += nn(spread[i], recv_x[i, k])
        for h, v in enumerate(halves(acc[:half], acc[half:])):
            send_y[2 * quarter(k) + h] = v.astype(BF16)
        for h in (0, 1):
            if (k, h) in y_copies:
                col_copy(k, h).start()
    recv_y[y] = send_y[y]
    served(groups - 1)
    with jax.named_scope("drain"):
        drain()

    with jax.named_scope("await_act"):
        plane_done(acts, sem_act)
    shared = tn(acts[...].reshape(n_tp * per_j, tokens), sdown[...])
    mixed = halves(shared[:half], shared[half:])[0]
    with jax.named_scope("await_y"):
        for k, h in y_copies:
            col_arrival(k, h).wait_recv()
    for i in range(n_y):
        mixed += recv_y[i].astype(F32)
    mixed = mixed.T
    o_mix[...] = jnp.concatenate([mixed[:64], mixed[64:]], axis=1).astype(BF16)

    sent(send_y.at[pl.ds(0, n_y - 1)], sem_y_s)


def deliver(*refs):
    n = (len(refs) - 1) // 2
    copies = []
    for i in range(n):
        parts = range(refs[i].shape[0]) if i < 3 else (None,)
        for g in parts:
            ends = [ref if g is None else ref.at[g] for ref in (refs[i], refs[n + i])]
            copies.append(pltpu.make_async_copy(*ends, refs[-1].at[len(copies)]))
    for copy in copies:
        copy.start()
    for copy in copies:
        copy.wait()


def on_device(*args):
    n_tp, units = args[0].shape[:2]
    nz = lax.axis_size("fs") // 2
    tokens, width = args[7].shape
    top = args[8].shape[1]
    cap = min(tokens, 5 * tokens * top // (2 * n_tp))
    hidden = nz * 2 * units
    per_j = -(-hidden // (16 * n_tp)) * 16
    n_y = n_tp // NX
    far = nz // 2
    groups = nz // 4
    args = [jnp.swapaxes(v, 0, 1) for v in args[:3]] + list(args[3:])
    args[6] = args[6].reshape(1, -1)
    args[8:] = [v.T for v in args[8:]]
    vm = pl.BlockSpec(memory_space=pltpu.VMEM)
    hbm = pl.BlockSpec(memory_space=pl.ANY)
    dma = pltpu.SemaphoreType.DMA
    big = pltpu.VMEM((groups, 8 * units, width), BF16)
    thin = pltpu.VMEM((64, hidden), BF16)
    mix = pltpu.VMEM((64, tokens), BF16)
    outs = pl.pallas_call(
        functools.partial(kernel, n_tp, nz, units, cap),
        name="hand_over",
        out_shape=[big, big, big, thin, thin, thin, mix],
        in_specs=[hbm] * 10,
        out_specs=[vm] * 7,
        scratch_shapes=[
            *[pltpu.VMEM(v.shape, v.dtype) for v in args],
            pltpu.VMEM((n_tp, ROW // 2, 128), F32),
            pltpu.VMEM((24 * units, 8 * ROW), BF16),
            pltpu.VMEM((2, n_tp, PIECE, 128), BF16),
            pltpu.VMEM((2, n_tp, PIECE, 128), BF16),
            pltpu.VMEM((nz, 2, ROW, width), BF16),
            pltpu.VMEM((nz, 2, ROW // 2, 128), BF16),
            pltpu.VMEM((tokens, width), BF16),
            pltpu.VMEM((cap, width), BF16),
            pltpu.VMEM((cap, width), F32),
            pltpu.VMEM((NX, tokens, cap), BF16),
            pltpu.VMEM((cap, 128), F32),
            pltpu.VMEM((n_tp, per_j, 128), BF16),
            pltpu.VMEM((n_tp, per_j, 128), BF16),
            pltpu.VMEM((n_tp, per_j, tokens), BF16),
            pltpu.VMEM((n_tp * per_j, 128), BF16),
            pltpu.VMEM((NX, n_y // 2, cap, 128), BF16),
            pltpu.VMEM((NX, n_y // 2, cap, 128), BF16),
            pltpu.VMEM((n_y, tokens // 2, 128), BF16),
            pltpu.VMEM((n_y, tokens // 2, 128), BF16),
            dma((10,)),
            dma((4,)),
            dma((2, len(ORDER))),
            dma((2, far, len(ORDER))),
            dma(()),
            dma((nz,)),
            dma((2,)),
            dma((2, far)),
            dma((2,)),
            dma((2,)),
            dma((2,)),
            dma(()),
            dma((n_y // 2, NX)),
            dma(()),
            dma((n_y // 2, 2)),
        ],
        compiler_params=pltpu.CompilerParams(
            collective_id=0, has_side_effects=True, vmem_limit_bytes=56 * 1024 * 1024
        ),
    )(*args)
    outs = pl.pallas_call(
        deliver,
        name="deliver",
        out_shape=[jax.ShapeDtypeStruct(v.shape, v.dtype) for v in outs],
        in_specs=[vm] * 7,
        out_specs=[hbm] * 7,
        scratch_shapes=[dma((3 * groups + 4,))],
        compiler_params=pltpu.CompilerParams(vmem_limit_bytes=1024 * 1024),
    )(*[pltpu.with_memory_space_constraint(v, pltpu.VMEM) for v in outs])
    full = [v.reshape(1, hidden, width) for v in outs[:3]]
    return (*full, *[v.T for v in outs[3:]])


def solution(mesh):
    placed = (
        P(None, "fs", "tp"),
        P(None, "fs", "tp"),
        P(None, "fs", "tp"),
        P("fs", "tp"),
        P("fs", "tp"),
        P("fs", "tp"),
        P("tp"),
        P("fs", None),
        P("fs", None),
        P("fs", None),
    )
    return jax.shard_map(
        on_device,
        mesh=mesh,
        in_specs=placed,
        out_specs=(
            P("tp", None, None),
            P("tp", None, None),
            P("tp", None, None),
            P(None, "tp"),
            P(None, "tp"),
            P(None, "tp"),
            P("fs", "tp"),
        ),
        check_vma=False,
    )
```

```python
import functools

import jax
import jax.numpy as jnp
from jax import lax
from jax.experimental import pallas as pl
from jax.experimental.pallas import tpu as pltpu
from jax.sharding import PartitionSpec as P

EPSILON = 1e-06
ROUTED_SCALE = 2.5
MESH = pl.DeviceIdType.MESH
NX = 4
ROW = 64
PIECE = 16
ORDER = (0, 2, 1, 3)
F32, BF16 = jnp.float32, jnp.bfloat16


def nt(a, b):
    return lax.dot_general(a, b, (((1,), (1,)), ((), ())), preferred_element_type=F32)


def tn(a, b):
    return lax.dot_general(a, b, (((0,), (0,)), ((), ())), preferred_element_type=F32)


def nn(a, b):
    return jnp.dot(a, b, preferred_element_type=F32)


def iota(shape, dim):
    return lax.broadcasted_iota(jnp.int32, shape, dim)


def silu(v):
    return v / (1.0 + jnp.exp(-v))


def halves(a, b):
    low = iota(a.shape, len(a.shape) - 1) < 64
    ax = len(a.shape) - 1
    return (
        jnp.where(low, a, pltpu.roll(b, 64, ax)),
        jnp.where(low, pltpu.roll(a, 64, ax), b),
    )


def kernel(
    n_tp, nz, units, cap,
    *refs,
):
    hbm_in, refs = refs[:10], refs[10:]
    outs, refs = refs[:7], refs[7:]
    inputs, refs = refs[:10], refs[10:]
    body(n_tp, nz, units, cap, hbm_in, *inputs, *outs, *refs)


def body(
    n_tp, nz, units, cap, hbm_in,
    tg, tu, td, sg, su, sd, gain, tok, ids, scores,
    o_gate, o_up, o_down, o_sgate, o_sup, o_sdown, o_mix,
    packed, pick, send_a, recv_a, blocks, small, normed, rows, total, spread, slot_weight,
    pre_send, pre_recv, acts, sdown, send_x, recv_x, send_y, recv_y,
    sem_in, sem_a, sem_ring_s, sem_ring_r, sem_pair_s, sem_pair_r,
    sem_small_s, sem_small_r, sem_spair, sem_j, sem_act, sem_x_s, sem_x_r, sem_y_s, sem_y_r,
):
    n_y = n_tp // NX
    far = nz // 2
    groups = nz // 4
    group_rows = 8 * units
    hidden = nz * 2 * units
    per_j = pre_send.shape[1]
    width = total.shape[1]
    tokens = tok.shape[0]
    me = lax.axis_index("tp")
    fs = lax.axis_index("fs")
    z, core = fs // 2, lax.rem(fs, 2)
    y, x = me // NX, lax.rem(me, NX)
    ahead = lax.rem(z + 1, nz) * 2 + core
    behind = lax.rem(z + nz - 1, nz) * 2 + core
    twin = z * 2 + 1 - core

    barrier = pltpu.get_barrier_semaphore()

    away = [(min(i, n_y - i) + min(j, NX - j), i, j) for i in range(n_y) for j in range(NX)]
    away = [
        lax.rem(y + i, n_y) * NX + lax.rem(x + j, NX)
        for distance, i, j in sorted(away, reverse=True)
        if distance
    ]
    vmem_in = (tg, tu, td, sg, su, sd, gain, tok, ids, scores)
    loads = [pltpu.make_async_copy(hbm_in[i], vmem_in[i], sem_in.at[i]) for i in range(10)]
    for load in loads:
        load.start()
    for other in (ahead, behind, twin):
        pl.semaphore_signal(barrier, inc=1, device_id={"fs": other}, device_id_type=MESH)
    for peer in away:
        pl.semaphore_signal(barrier, inc=1, device_id={"tp": peer}, device_id_type=MESH)
    for i in (0, 1, 2, 3, 4, 5, 6):
        loads[i].wait()

    scale = gain[...]

    with jax.named_scope("pack"):

        def unit(r):
            if r < units:
                return tg[r] * scale
            if r < 2 * units:
                return tu[r - units] * scale
            return td[r - 2 * units] if r < 3 * units else jnp.zeros((n_tp, 64), F32)

        parts = [sg[...] * scale, su[...] * scale, sd[...]]
        stack = jnp.concatenate([*parts, jnp.zeros((ROW - 3 * units, 64), F32)], axis=0)
        stack = jnp.concatenate([stack[: ROW // 2], stack[ROW // 2 :]], axis=1)
        small[z, core] = stack.astype(BF16)
        for r in range(0, ROW // 2, 8):
            several = [
                jnp.concatenate([unit(i), unit(i + ROW // 2)], axis=1) for i in range(r, r + 8)
            ]
            packed[:, pl.ds(r, 8), :] = jnp.swapaxes(jnp.stack(several, axis=0), 0, 1)
        for h in (0, 1):
            send_a[h] = packed[:, pl.ds(PIECE * h, PIECE), :].astype(BF16)
            recv_a[h, me] = send_a[h, me]
    with jax.named_scope("entry"):
        pl.semaphore_wait(barrier, n_tp + 2)

    def plane(src, dst, sems, peer, at=0):
        return pltpu.make_async_remote_copy(
            src_ref=src, dst_ref=dst, send_sem=sems.at[at], recv_sem=sems.at[at + 1],
            device_id={"tp": peer}, device_id_type=MESH,
        )

    def plane_done(ref, sems, at=0):
        piece = ref.at[pl.ds(0, n_tp - 1)]
        done = plane(piece, piece, sems, lax.rem(me + 1, n_tp), at)
        done.wait_send()
        done.wait_recv()

    def small_hop(d, s, at):
        return pltpu.make_async_remote_copy(
            src_ref=small.at[at, core], dst_ref=small.at[at, core],
            send_sem=sem_small_s.at[d], recv_sem=sem_small_r.at[d, s - 1],
            device_id={"fs": ahead if d == 0 else behind}, device_id_type=MESH,
        )

    def small_pair(at):
        return pltpu.make_async_remote_copy(
            src_ref=small.at[at, core], dst_ref=small.at[at, core],
            send_sem=sem_spair.at[0], recv_sem=sem_spair.at[1],
            device_id={"fs": twin}, device_id_type=MESH,
        )

    def origin(d, s):
        return lax.rem(z + nz - s, nz) if d == 0 else lax.rem(z + s, nz)

    small_hop(0, 1, z).start()
    small_hop(1, 1, z).start()
    small_pair(z).start()

    for h in (0, 1):
        for peer in away:
            plane(send_a.at[h, peer], recv_a.at[h, me], sem_a, peer, 2 * h).start()

    def small_step(s):
        for d in (0, 1):

            def arrived(d=d):
                at = origin(d, s)
                small_hop(d, s, at).wait_recv()
                small_pair(at).start()

                @pl.when((s + 1 < far) | ((s + 1 == far) & (d == 0)))
                def _():
                    small_hop(d, s + 1, at).start()

            if d == 0:
                arrived()
            else:
                pl.when(s < far)(arrived)

    for i in (7, 8, 9):
        loads[i].wait()
    tf = tok[...].astype(F32)
    normed[...] = (
        tf * lax.rsqrt(jnp.mean(tf * tf, axis=1, keepdims=True) + EPSILON)
    ).astype(BF16)
    ids_v, sc = ids[...], scores[...]
    ratio = ROUTED_SCALE * sc / jnp.sum(sc, axis=0, keepdims=True)
    expert_row = iota((128, tokens), 0)
    present = jnp.zeros((128, tokens), F32)
    weight_row = jnp.zeros((1, tokens), F32)
    for k in range(ids.shape[0]):
        present = jnp.where(ids_v[k : k + 1] == expert_row, 1.0, present)
        weight_row += jnp.where(ids_v[k : k + 1] == me, ratio[k : k + 1], 0.0)
    before = jnp.where(iota((tokens, tokens), 0) < iota((tokens, tokens), 1), 1.0, 0.0)
    position = nn(present.astype(BF16), before.astype(BF16))
    slots = jnp.where(present > 0.0, position, -1.0)
    slot_row = jnp.sum(jnp.where(expert_row == me, slots, 0.0), axis=0, keepdims=True)
    slot = slots.T
    lane = iota((tokens, 128), 1)
    taken = slot_row == iota((cap, tokens), 0).astype(F32)
    slot_weight[...] = jnp.broadcast_to(
        jnp.sum(jnp.where(taken, weight_row, 0.0), axis=1, keepdims=True), slot_weight.shape
    )
    rows[...] = nn(jnp.where(taken, 1.0, 0.0).astype(BF16), normed[...]).astype(BF16)
    for i in range(NX):
        col = jnp.sum(jnp.where(lane == y * NX + i, slot, 0.0), axis=1, keepdims=True)
        spread[i] = jnp.where(col == iota((tokens, cap), 1).astype(F32), 1.0, 0.0).astype(BF16)
    total[...] = jnp.zeros_like(total)

    shape = (group_rows, 8 * ROW)
    i, f, r = iota(shape, 0), iota(shape, 1) // ROW, iota(shape, 1) & (ROW - 1)
    ordered = []
    for m in range(3):
        inside = (r >= units * m) & (r < units * (m + 1))
        ordered.append(jnp.where(inside & (i == units * f + r - units * m), 1.0, 0.0))
    pick[...] = jnp.concatenate(ordered, axis=0).astype(BF16)

    def hop(d, s, q, at):
        piece = blocks.at[at, core, pl.ds(q * PIECE, PIECE)]
        return pltpu.make_async_remote_copy(
            src_ref=piece, dst_ref=piece,
            send_sem=sem_ring_s.at[d, q], recv_sem=sem_ring_r.at[d, s - 1, q],
            device_id={"fs": ahead if d == 0 else behind}, device_id_type=MESH,
        )

    def pair(at, q=None):
        block = blocks.at[at, core]
        piece = block if q is None else blocks.at[at, core, pl.ds(q * PIECE, PIECE)]
        return pltpu.make_async_remote_copy(
            src_ref=piece, dst_ref=piece,
            send_sem=sem_pair_s, recv_sem=sem_pair_r.at[lax.rem(at + nz - z, nz)],
            device_id={"fs": twin}, device_id_type=MESH,
        )

    early = 3
    with jax.named_scope("small_early"):
        for i in range(1, early):
            small_step(i)
    for h in (0, 1):
        if h:
            with jax.named_scope("small_between"):
                small_step(early)
        with jax.named_scope(f"await_weights{h}"):
            plane_done(recv_a.at[h], sem_a, 2 * h)
        with jax.named_scope("unpack"):
            for m in range(n_tp // 2):
                upper, lower = recv_a[h, 2 * m].astype(F32), recv_a[h, 2 * m + 1].astype(F32)
                for part, v in enumerate(halves(upper, lower)):
                    at = pl.ds(PIECE * (h + 2 * part), PIECE)
                    blocks[z, core, at, pl.ds(128 * m, 128)] = v.astype(BF16)
        for q in ORDER[2 * h : 2 * h + 2]:
            for d in (0, 1):
                hop(d, 1, q, z).start()
            pair(z, q).start()

    def last_leg(d, q):
        return (q in ORDER[:2]) == (d == 0)

    def activated(*ats):
        with jax.named_scope("await_pair"):
            for at in ats:
                pair(at).wait_recv()
        w = jnp.concatenate([blocks[at].reshape(2 * ROW, width) for at in ats], axis=0)
        pre = nt(rows[...], w)
        act = silu(pltpu.roll(pre, 2 * units, 1)) * pltpu.roll(pre, units, 1)
        unit = iota(act.shape, 1) & (ROW - 1)
        return jnp.where((unit >= 2 * units) & (unit < 3 * units), act, 0.0).astype(BF16)

    def expert(*ats):
        act = activated(*ats)
        w = jnp.concatenate([blocks[at].reshape(2 * ROW, width) for at in ats], axis=0)
        total[...] += nn(act, w)

    def padded(v):
        spare = jnp.zeros((-hidden % 128, 128), F32)
        return jnp.concatenate([v, spare], axis=0)

    def shared_rows():
        got = [[], [], []]
        for g in range(groups):
            v = small[pl.ds(4 * g, 4)].reshape(8, ROW // 2, 128).astype(F32)
            v = jnp.concatenate([v, pltpu.roll(v, 64, 2)], axis=1).reshape(8 * ROW, 128)
            v = v.astype(BF16)
            found = nn(pick[...], v)
            for m in range(3):
                got[m].append(found[group_rows * m : group_rows * (m + 1)])
        gate, up, down = [jnp.concatenate(one, axis=0) for one in got]
        for o, v in ((o_sgate, gate), (o_sup, up), (o_sdown, down)):
            o[...] = padded(v).T[:64, :hidden].astype(BF16)
        pad = jnp.zeros((n_tp * per_j - hidden, 128), F32)
        both = jnp.concatenate([halves(gate, up)[0], pad], axis=0)
        pre_send[...] = both.astype(BF16).reshape(n_tp, per_j, 128)
        low = iota(down.shape, 1) < 64
        down = jnp.concatenate([jnp.where(low, down, 0.0), pad], axis=0)
        sdown[...] = down.astype(BF16)
        pre_recv[me] = pre_send[me]

        def send(i, _):
            peer = lax.rem(me + i, n_tp)
            plane(pre_send.at[peer], pre_recv.at[me], sem_j, peer).start()
            return 0

        lax.fori_loop(1, n_tp, send, 0)

    def shared_acts():
        with jax.named_scope("await_j"):
            plane_done(pre_recv, sem_j)
        gates, ups = [], []
        for m in range(n_tp // 2):
            g, u = halves(pre_recv[2 * m].astype(F32), pre_recv[2 * m + 1].astype(F32))
            gates.append(g.astype(BF16))
            ups.append(u.astype(BF16))
        gate = nt(jnp.concatenate(gates, axis=1), normed[...])
        up = nt(jnp.concatenate(ups, axis=1), normed[...])
        acts[me] = (silu(gate) * up).astype(BF16)

        def send_act(i, _):
            peer = lax.rem(me + i, n_tp)
            plane(acts.at[me], acts.at[me], sem_act, peer).start()
            return 0

        lax.fori_loop(1, n_tp, send_act, 0)

    def ring_step(s, _):
        for n, q in enumerate(ORDER):
            for d in (0, 1):
                at = origin(d, s)
                with jax.named_scope(f"arrive{d}{n}"):
                    hop(d, s, q, at).wait_recv()
                if last_leg(d, q):
                    hop(d, s + 1, q, at).start()
                else:

                    @pl.when(s + 1 < far)
                    def _(d=d, q=q, at=at):
                        hop(d, s + 1, q, at).start()

                pair(at, q).start()

            if n == 1:

                @pl.when(s + early <= far)
                def _():
                    with jax.named_scope("small"):
                        small_step(s + early)

            if n == 3:

                @pl.when(s == far - early)
                def _():
                    with jax.named_scope("await_small"):
                        everything = small.at[:, 0]
                        done = pltpu.make_async_remote_copy(
                            src_ref=everything, dst_ref=everything,
                            send_sem=sem_spair.at[0], recv_sem=sem_spair.at[1],
                            device_id={"fs": twin}, device_id_type=MESH,
                        )
                        done.wait_send()
                        done.wait_recv()
                    with jax.named_scope("shared_rows"):
                        shared_rows()

            if n == 2:

                @pl.when(s == far - 1)
                def _():
                    with jax.named_scope("expert_in"):
                        expert(origin(0, s - 1), origin(1, s - 1))

        @pl.when(s == 1)
        def _():
            with jax.named_scope("expert_own"):
                expert(z)

        @pl.when((s > 1) & (s < far - 1))
        def _():
            with jax.named_scope("expert"):
                expert(origin(0, s - 1), origin(1, s - 1))

        return 0

    lax.fori_loop(1, far, ring_step, 0)
    opposite = lax.rem(z + far, nz)
    with jax.named_scope("shared_acts"):
        shared_acts()

    def take_last():
        for q in (*ORDER[::2], *ORDER[1::2]):
            hop(0 if q in ORDER[:2] else 1, far, q, opposite).wait_recv()
            pair(opposite, q).start()

    pl.when(core == 1)(take_last)
    with jax.named_scope("expert_near"):
        expert(origin(0, far - 1), origin(1, far - 1))
    pl.when(core == 0)(take_last)
    with jax.named_scope("expert_last"):
        act = activated(opposite)

    def sent(ref, sem):
        pltpu.make_async_remote_copy(
            src_ref=ref, dst_ref=ref, send_sem=sem, recv_sem=sem_pair_r.at[0],
            device_id={"fs": twin}, device_id_type=MESH,
        ).wait_send()

    def drain():
        for d in (0, 1):
            for q in ORDER:
                hops = far - 1 + last_leg(d, q)
                sent(blocks.at[pl.ds(0, hops), 0, pl.ds(0, PIECE)], sem_ring_s.at[d, q])
            sent(small.at[pl.ds(0, far - d), 0], sem_small_s.at[d])
        sent(blocks.at[:, 0], sem_pair_s)
        sent(send_x.at[pl.ds(0, NX - 1)], sem_x_s)

    w = slot_weight[...]
    pairs = n_y // 2
    turns = [(pairs // 2 + (i + 1) // 2 * (1 if i % 2 else -1)) % pairs for i in range(pairs)]
    turns = [i for i in turns if i] + [0]

    def quarter(k):
        return lax.rem(y // 2 + turns[k], pairs)

    def row_copy(k, i):
        to = lax.rem(x + i, NX)
        return pltpu.make_async_remote_copy(
            src_ref=send_x.at[to, k], dst_ref=recv_x.at[x, k],
            send_sem=sem_x_s, recv_sem=sem_x_r.at[k, i],
            device_id={"tp": y * NX + to}, device_id_type=MESH,
        )

    for k in range(pairs):
        p = quarter(k)
        for h in range(NX // 2):
            several = []
            for i in (2 * p, 2 * p + 1):
                cols = pl.ds(pl.multiple_of(128 * (i * (NX // 2) + h), 128), 128)
                new = nn(act, blocks[opposite, :, :, cols].reshape(2 * ROW, 128))
                several.append((total[:, cols] + new) * w)
            for i, v in enumerate(halves(*several)):
                send_x[2 * h + i, k] = v.astype(BF16)
        for i in (2, 1, 3) if NX == 4 else range(1, NX):
            row_copy(k, i).start()
        recv_x[x, k] = send_x[x, k]

    part = min(512, width)
    results = (o_gate, o_up, o_down)

    def served(g):
        def some(n, _):
            cols = pl.ds(pl.multiple_of(n * part, part), part)
            v = blocks[pl.ds(4 * g, 4), :, :, cols].reshape(8 * ROW, part)
            v = nn(pick[...], v)
            for m in range(3):
                results[m][g, :, cols] = v[group_rows * m : group_rows * (m + 1)].astype(BF16)
            return 0

        with jax.named_scope("served"):
            lax.fori_loop(0, width // part, some, 0)

    for g in range(groups - 1):
        served(g)

    half = tokens // 2
    odd = lax.rem(y, 2)

    def col_copy(k, h):
        last = k == pairs - 1
        to = 2 * quarter(k) + (1 - odd if last else h)
        return pltpu.make_async_remote_copy(
            src_ref=send_y.at[to], dst_ref=recv_y.at[y],
            send_sem=sem_y_s, recv_sem=sem_y_r.at[k, 0 if last else odd],
            device_id={"tp": to * NX + x}, device_id_type=MESH,
        )

    def col_arrival(k, h):
        return pltpu.make_async_remote_copy(
            src_ref=recv_y.at[0], dst_ref=recv_y.at[0],
            send_sem=sem_y_s, recv_sem=sem_y_r.at[k, h],
            device_id={"tp": lax.rem(me + 1, n_tp)}, device_id_type=MESH,
        )

    y_copies = [(k, h) for k in range(pairs) for h in (0, 1) if k < pairs - 1 or h == 0]
    for k in range(pairs):
        acc = nn(spread[x], recv_x[x, k])
        for i in range(1, NX):
            row_copy(k, i).wait_recv()
            source = lax.rem(x + NX - i, NX)
            acc += nn(spread[source], recv_x[source, k])
        for h, v in enumerate(halves(acc[:half], acc[half:])):
            send_y[2 * quarter(k) + h] = v.astype(BF16)
        for h in (0, 1):
            if (k, h) in y_copies:
                col_copy(k, h).start()
    recv_y[y] = send_y[y]
    served(groups - 1)
    with jax.named_scope("drain"):
        drain()

    with jax.named_scope("await_act"):
        plane_done(acts, sem_act)
    shared = tn(acts[...].reshape(n_tp * per_j, tokens), sdown[...])
    mixed = halves(shared[:half], shared[half:])[0]
    with jax.named_scope("await_y"):
        for k, h in y_copies:
            col_arrival(k, h).wait_recv()
    for i in range(n_y):
        mixed += recv_y[i].astype(F32)
    mixed = mixed.T
    o_mix[...] = jnp.concatenate([mixed[:64], mixed[64:]], axis=1).astype(BF16)

    sent(send_y.at[pl.ds(0, n_y - 1)], sem_y_s)


def deliver(*refs):
    n = (len(refs) - 1) // 2
    copies = []
    for i in range(n):
        parts = range(refs[i].shape[0]) if i < 3 else (None,)
        for g in parts:
            ends = [ref if g is None else ref.at[g] for ref in (refs[i], refs[n + i])]
            copies.append(pltpu.make_async_copy(*ends, refs[-1].at[len(copies)]))
    for copy in copies:
        copy.start()
    for copy in copies:
        copy.wait()


def on_device(*args):
    n_tp, units = args[0].shape[:2]
    nz = lax.axis_size("fs") // 2
    tokens, width = args[7].shape
    top = args[8].shape[1]
    cap = min(tokens, 5 * tokens * top // (2 * n_tp))
    hidden = nz * 2 * units
    per_j = -(-hidden // (16 * n_tp)) * 16
    n_y = n_tp // NX
    far = nz // 2
    groups = nz // 4
    args = [jnp.swapaxes(v, 0, 1) for v in args[:3]] + list(args[3:])
    args[6] = args[6].reshape(1, -1)
    args[8:] = [v.T for v in args[8:]]
    vm = pl.BlockSpec(memory_space=pltpu.VMEM)
    hbm = pl.BlockSpec(memory_space=pl.ANY)
    dma = pltpu.SemaphoreType.DMA
    big = pltpu.VMEM((groups, 8 * units, width), BF16)
    thin = pltpu.VMEM((64, hidden), BF16)
    mix = pltpu.VMEM((64, tokens), BF16)
    outs = pl.pallas_call(
        functools.partial(kernel, n_tp, nz, units, cap),
        name="hand_over",
        out_shape=[big, big, big, thin, thin, thin, mix],
        in_specs=[hbm] * 10,
        out_specs=[vm] * 7,
        scratch_shapes=[
            *[pltpu.VMEM(v.shape, v.dtype) for v in args],
            pltpu.VMEM((n_tp, ROW // 2, 128), F32),
            pltpu.VMEM((24 * units, 8 * ROW), BF16),
            pltpu.VMEM((2, n_tp, PIECE, 128), BF16),
            pltpu.VMEM((2, n_tp, PIECE, 128), BF16),
            pltpu.VMEM((nz, 2, ROW, width), BF16),
            pltpu.VMEM((nz, 2, ROW // 2, 128), BF16),
            pltpu.VMEM((tokens, width), BF16),
            pltpu.VMEM((cap, width), BF16),
            pltpu.VMEM((cap, width), F32),
            pltpu.VMEM((NX, tokens, cap), BF16),
            pltpu.VMEM((cap, 128), F32),
            pltpu.VMEM((n_tp, per_j, 128), BF16),
            pltpu.VMEM((n_tp, per_j, 128), BF16),
            pltpu.VMEM((n_tp, per_j, tokens), BF16),
            pltpu.VMEM((n_tp * per_j, 128), BF16),
            pltpu.VMEM((NX, n_y // 2, cap, 128), BF16),
            pltpu.VMEM((NX, n_y // 2, cap, 128), BF16),
            pltpu.VMEM((n_y, tokens // 2, 128), BF16),
            pltpu.VMEM((n_y, tokens // 2, 128), BF16),
            dma((10,)),
            dma((4,)),
            dma((2, len(ORDER))),
            dma((2, far, len(ORDER))),
            dma(()),
            dma((nz,)),
            dma((2,)),
            dma((2, far)),
            dma((2,)),
            dma((2,)),
            dma((2,)),
            dma(()),
            dma((n_y // 2, NX)),
            dma(()),
            dma((n_y // 2, 2)),
        ],
        compiler_params=pltpu.CompilerParams(
            collective_id=0, has_side_effects=True, vmem_limit_bytes=56 * 1024 * 1024
        ),
    )(*args)
    outs = pl.pallas_call(
        deliver,
        name="deliver",
        out_shape=[jax.ShapeDtypeStruct(v.shape, v.dtype) for v in outs],
        in_specs=[vm] * 7,
        out_specs=[hbm] * 7,
        scratch_shapes=[dma((3 * groups + 4,))],
        compiler_params=pltpu.CompilerParams(vmem_limit_bytes=1024 * 1024),
    )(*[pltpu.with_memory_space_constraint(v, pltpu.VMEM) for v in outs])
    full = [v.reshape(1, hidden, width) for v in outs[:3]]
    return (*full, *[v.T for v in outs[3:]])


def solution(mesh):
    placed = (
        P(None, "fs", "tp"),
        P(None, "fs", "tp"),
        P(None, "fs", "tp"),
        P("fs", "tp"),
        P("fs", "tp"),
        P("fs", "tp"),
        P("tp"),
        P("fs", None),
        P("fs", None),
        P("fs", None),
    )
    return jax.shard_map(
        on_device,
        mesh=mesh,
        in_specs=placed,
        out_specs=(
            P("tp", None, None),
            P("tp", None, None),
            P("tp", None, None),
            P(None, "tp"),
            P(None, "tp"),
            P(None, "tp"),
            P("fs", "tp"),
        ),
        check_vma=False,
    )
```
